1024 devices in a mesh: grp: 2 (over x), fs: 16 (over z), tp: 32 (over y, core).
Axes of the slice: x: 2, y: 16, z: 16, core: 2. Of those that a mesh axis runs over, the one named last changes fastest.
The devices are a block of a 4x16x16 slice.
Arguments:
- tokens: bfloat16 [8192, 2048], P(('grp', 'fs')), parts along dimension 0, may hold values from -6 to 6
- routes: int32 [8192, 2], P(('grp', 'fs')), parts along dimension 0, may hold values from 0 to 15, all different within a row; in each aligned block of 256 rows (0 to 255, 256 to 511, ...) at most 48 rows name the same one
- route_logits: float32 [8192, 2], P(('grp', 'fs')), parts along dimension 0, may hold values from -6 to 6
- gain: float32 [2048], P('fs'), may hold values from 0.1 to 1.9
- w_gate: float32 [16, 2048, 4096], P(None, 'fs', 'tp'), may hold values from -0.125 to 0.125
- w_up: float32 [16, 2048, 4096], P(None, 'fs', 'tp'), may hold values from -0.125 to 0.125
- w_down: float32 [16, 2048, 4096], P(None, 'fs', 'tp'), may hold values from -0.09375 to 0.09375
Outputs:
- gate_out: bfloat16 [32, 2048, 4096], P(('grp', 'fs'), None, 'tp'), parts along dimension 0
- up_out: bfloat16 [32, 2048, 4096], P(('grp', 'fs'), None, 'tp'), parts along dimension 0
- down_out: bfloat16 [32, 2048, 4096], P(('grp', 'fs'), None, 'tp'), parts along dimension 0
- mixed: bfloat16 [8192, 2048], P(('grp', 'fs'), 'tp'), parts along dimension 0
The draws below stay inside these ranges and needn't reach their ends.
There are 2 independent parts, one for each index of `grp`. The reference program is written for one: setup_inputs(seed, part) draws one part's arguments, and reference() takes and returns one part's arrays. A program takes and returns all parts, laid end to end along the dimension named above; an argument that names none is the same for every part. Nothing has to cross between parts.
Inputs may be any that keep to these rules, and one draw needn't show every extreme that they name: `routes`: each row names two different experts. In each aligned block of 256 rows (the tokens of one index of fs) no expert is named by more than 48 rows, a bound that some block reaches.
All inputs are finite; a program needn't handle non-finite values.
Results may differ from the reference program's by a relative error of at most 0.025.
Values may be sent and summed in bfloat16 or wider, within the bound.
A program may use at most 32 MiB of HBM per device.

```python
import math
import jax
import jax.numpy as jnp
import numpy as np
from jax import lax

D = 2048
FF = 4096
E = 16
TOK_DEV = 256
CAP = 48
TOKENS = 4096
N_FS = 16
N_TP = 32


def steps_of(rng, dims, split, smallest, largest):
    level, own = 1.0, jax.random.fold_in(rng, 6)
    for position, parts in split:
        steps = jnp.exp(jax.random.uniform(jax.random.fold_in(own, position), (parts,), jnp.float32, smallest / len(split), largest / len(split)))
        level = level * jnp.repeat(steps, dims[position] // parts).reshape([-1 if axis == position else 1 for axis in range(len(dims))])
    return level


def shared_out(key, own, number, rows, count, top, reach, lean):
    ranking = jax.random.permutation(key, count)
    crowded, usual = load_shares(count, rows * top, reach, lean, True), load_shares(count, rows * top, reach, lean, False)
    places = jnp.arange(count)

    def named(lengths, rotation):
        used = int((lengths > 0).sum())
        fixed = max(1, used // 4)
        shifted = fixed + (places - fixed + rotation * (used - fixed)) % max(1, count - fixed)
        return jnp.zeros((count,), jnp.int32).at[ranking[jnp.where(places < fixed, places, shifted)]].set(jnp.asarray(lengths, jnp.int32))

    lengths = jnp.where(number % 4 == 0, named(crowded, number // 4), named(usual, number - number // 4 - 1))
    mixed = jax.random.permutation(jax.random.fold_in(own, 3), count)
    source_of, sink = mixed[0:count // 2 * 2:2], mixed[1:count // 2 * 2:2]
    margin = jnp.minimum(lengths[source_of] - 1, reach - lengths[sink]) // 2
    margin = jnp.where((source_of == ranking[0]) | (sink == ranking[0]) | (lengths[sink] == 0), 0, jnp.maximum(margin, 0))
    shifted = jax.random.randint(jax.random.fold_in(own, 4), (count // 2,), 0, 1 << 20) % (margin + 1)
    lengths = lengths.at[source_of].add(-shifted).at[sink].add(shifted)
    members = jnp.searchsorted(jnp.cumsum(lengths), jnp.arange(rows * top), side="right").astype(jnp.int32)
    grid = members.reshape(top, rows).T
    grid = grid[jax.random.permutation(jax.random.fold_in(own, 1), rows)]
    rotation = jax.random.randint(jax.random.fold_in(own, 2), (rows, 1), 0, top)
    return jnp.take_along_axis(grid, (jnp.arange(top)[None, :] + rotation) % top, axis=1)


def load_shares(number_of, total, reach, slope, full):
    loads = [(1 << 20) // math.isqrt(rank ** slope) + 1 for rank in range(1, number_of + 1)]
    largest = reach if full else min(reach, max(-(-total // number_of), total * loads[0] // sum(loads)))
    least = 1 if total - largest >= number_of - 1 else 0
    counts, surplus = [largest] + [least] * (number_of - 1), total - largest - least * (number_of - 1)
    while surplus > 0:
        movable = [i for i in range(1, number_of) if counts[i] < largest] or [i for i in range(1, number_of) if counts[i] < reach]
        mass, budget = sum([loads[i] for i in movable]), surplus
        for i in movable:
            addition = min(reach - counts[i], max(1, budget * loads[i] // mass), surplus)
            counts[i] = counts[i] + addition
            surplus = surplus - addition
    return np.array(counts)


def gaussian(key, dims, scale, reach, shards=(), kind=jnp.bfloat16):
    level = steps_of(key, dims, shards, -0.22, 0.18) if shards else 1.0
    values = jax.random.normal(key, dims, jnp.float32) * scale * level
    return jnp.minimum(jnp.maximum(values, -reach), reach).astype(kind)


def setup_inputs(seed: int = 0, part: int = 0) -> dict:
    key_of = jax.random.split(jax.random.key(seed), 8)
    own_keys = jax.random.split(jax.random.fold_in(key_of[7], part), 8)
    tokens = gaussian(own_keys[0], (TOKENS, D), 1.0, 6.0, ((0, 16),))
    routes_keys = jax.random.split(jax.random.fold_in(own_keys[1], 1), TOKENS // TOK_DEV)
    routes_turns = jax.random.permutation(jax.random.fold_in(own_keys[1], 3), TOKENS // TOK_DEV)
    routes = jax.vmap(lambda own, number: shared_out(jax.random.fold_in(own_keys[1], 2), own, number, TOK_DEV, E, 2, CAP, 2))(routes_keys, routes_turns).reshape((TOKENS, 2))
    route_logits = gaussian(own_keys[2], (TOKENS, 2), 1.5, 6.0, ((0, 16),), jnp.float32)
    gain = jnp.clip(1.0 + 0.18 * jax.random.normal(key_of[3], (D,), jnp.float32), 0.1, 1.9)
    w_gate = gaussian(key_of[4], (E, D, FF), D ** -0.5, 0.125, ((1, 16), (2, 32)), jnp.float32)
    w_up = gaussian(key_of[5], (E, D, FF), D ** -0.5, 0.125, ((1, 16), (2, 32)), jnp.float32)
    w_down = gaussian(key_of[6], (E, D, FF), FF ** -0.5, 0.09375, ((1, 16), (2, 32)), jnp.float32)
    return dict(tokens=tokens, routes=routes, route_logits=route_logits, gain=gain, w_gate=w_gate, w_up=w_up, w_down=w_down)


EPS = 1e-06

def normalize(tokens):
    values = tokens.astype(jnp.float32)
    centred = values - lax.optimization_barrier(jnp.mean(values, axis=-1, keepdims=True))
    spread = lax.optimization_barrier(jnp.mean(centred * centred, axis=-1, keepdims=True))
    return (centred * lax.rsqrt(spread + EPS)).astype(jnp.bfloat16)

def route_shares(route_logits):
    diff = route_logits[:, 0] - route_logits[:, 1]
    return jax.nn.sigmoid(jnp.stack([diff, -diff], axis=1))

def reference(tokens, routes, route_logits, gain, w_gate, w_up, w_down):
    gate_out = (gain[None, :, None] * w_gate).astype(jnp.bfloat16)
    up_out = (gain[None, :, None] * w_up).astype(jnp.bfloat16)
    down_out = w_down.astype(jnp.bfloat16)
    normed = normalize(tokens)
    experts = jnp.arange(E, dtype=jnp.int32)
    chosen = routes[:, :, None] == experts[None, None, :]
    marked = lax.optimization_barrier(jnp.sum(chosen.astype(jnp.int32), axis=1))
    blocks = marked.reshape(N_FS, TOK_DEV, E)
    before = (jnp.cumsum(blocks, axis=1) - blocks).reshape(N_FS * TOK_DEV, E)
    source = jnp.arange(N_FS * TOK_DEV, dtype=jnp.int32) // TOK_DEV
    slot_ids = jnp.where(marked > 0, source[:, None] * CAP + before, -1).astype(jnp.int32)
    shares = route_shares(route_logits)
    weight_table = lax.optimization_barrier(jnp.sum(chosen.astype(jnp.float32) * shares[:, :, None], axis=1))
    places = jnp.arange(N_FS * CAP, dtype=jnp.int32)

    def one_expert(running, inputs):
        gate_w, up_w, down_w, slot_e, weight_e = inputs
        picker = places[:, None] == slot_e[None, :]
        routed = jnp.dot(picker.astype(jnp.bfloat16), normed, preferred_element_type=jnp.float32).astype(jnp.bfloat16)
        gate_sum = jnp.dot(routed, gate_w, preferred_element_type=jnp.float32)
        up_sum = jnp.dot(routed, up_w, preferred_element_type=jnp.float32)
        hidden = (jax.nn.silu(gate_sum) * up_sum).astype(jnp.bfloat16)
        hidden_blocks = hidden.astype(jnp.float32).reshape(N_FS * CAP, N_TP, FF // N_TP)
        down_blocks = down_w.astype(jnp.float32).reshape(D, N_TP, FF // N_TP)
        partial_value = jnp.einsum('rjh,djh->jrd', hidden_blocks, down_blocks).astype(jnp.bfloat16)
        result = lax.optimization_barrier(jnp.sum(partial_value.astype(jnp.float32), axis=0)).astype(jnp.bfloat16)
        spread_back = picker.astype(jnp.float32).T * weight_e[:, None]
        running = running + jnp.dot(spread_back, result.astype(jnp.float32), precision=lax.Precision.HIGHEST)
        return (running, None)
    running, _ = lax.scan(one_expert, jnp.zeros((N_FS * TOK_DEV, D), jnp.float32), (gate_out, up_out, down_out, slot_ids.T, weight_table.T))
    return (gate_out, up_out, down_out, running.astype(jnp.bfloat16))
```

```python
import functools

import jax
import jax.numpy as jnp
from jax import lax
from jax.experimental import pallas as pl
from jax.experimental.pallas import tpu as pltpu
from jax.sharding import PartitionSpec as P

EPS = 1e-06
MESH = pl.DeviceIdType.MESH
F32 = jnp.float32
BF16 = jnp.bfloat16


def loop(lo, hi, body):
    def step(i, carry):
        body(i)
        return carry

    lax.fori_loop(lo, hi, step, 0)


def kernel(
    dims,
    tokens_hbm,
    routes_ref,
    logits_ref,
    gain_ref,
    wg_hbm,
    wu_hbm,
    wd_hbm,
    go_hbm,
    uo_hbm,
    do_hbm,
    mix_ref,
    tok_v,
    normed_v,
    wf,
    wsend,
    wown,
    wpart,
    xb,
    dsend,
    pick,
    hid,
    acc_g,
    acc_u,
    part_r,
    part_l,
    rs_rsend,
    rs_lsend,
    rs_rrecv,
    rs_lrecv,
    ret_send,
    ret_recv,
    mix_own,
    mix_other,
    load_sem,
    store_sem,
    tok_s,
    tok_r,
    z_s,
    z_r,
    x_s,
    x_r,
    d_s,
    d_r,
    agr_s,
    agr_r,
    agl_s,
    agl_r,
    rsr_s,
    rsr_r,
    rsl_s,
    rsl_r,
    ret_s,
    ret_r,
    mix_s,
    mix_r,
):
    G, F, Y, cap, nsub = dims
    half = F // 2
    per = half // nsub
    right_steps, left_steps = Y // 2, Y // 2 - 1
    rows = wsend.shape[2]
    share = rows // G
    feats = xb.shape[3]

    g = lax.axis_index("grp")
    me = lax.axis_index("fs")
    t = lax.axis_index("tp")
    y = lax.div(t, 2)
    c = lax.rem(t, 2)
    partner = t + 1 - 2 * c
    right = lax.rem(y + 1, Y) * 2 + c
    left = lax.rem(y + Y - 1, Y) * 2 + c
    par = lax.rem(me + c, 2)

    def offset(m):
        step = lax.div(m + 1, 2)
        odd = lax.rem(m, 2)
        return odd * step + (1 - odd) * (F - step)

    barrier = pltpu.get_barrier_semaphore()

    def greet(m):
        pl.semaphore_signal(
            barrier, inc=1, device_id={"fs": lax.rem(me + m, F)}, device_id_type=MESH
        )

    loop(1, F, greet)
    for m in range(1, G):
        pl.semaphore_signal(
            barrier, inc=1, device_id={"grp": lax.rem(g + m, G)}, device_id_type=MESH
        )
    for other in (partner, left, right):
        pl.semaphore_signal(barrier, inc=1, device_id={"tp": other}, device_id_type=MESH)

    loads = [pltpu.make_async_copy(tokens_hbm, tok_v, load_sem.at[0])]
    for p, ref in enumerate((wg_hbm, wu_hbm, wd_hbm)):
        loads.append(pltpu.make_async_copy(ref, wf.at[p], load_sem.at[p + 1]))
    for copy in loads:
        copy.start()

    tok = tok_v.shape[0]
    lanes = 128
    experts = lax.broadcasted_iota(jnp.int32, (tok, lanes), 1)
    first = routes_ref[:, 0:1]
    second = routes_ref[:, 1:2]
    is_first = first == experts
    is_second = second == experts
    marked = jnp.where(is_first | is_second, 1.0, 0.0).astype(BF16)
    earlier = jnp.where(
        lax.broadcasted_iota(jnp.int32, (tok, tok), 1)
        < lax.broadcasted_iota(jnp.int32, (tok, tok), 0),
        1.0,
        0.0,
    ).astype(BF16)
    before = jnp.dot(earlier, marked, preferred_element_type=F32)
    key_first = first.astype(F32) * cap + jnp.sum(
        jnp.where(is_first, before, 0.0), axis=1, keepdims=True
    )
    key_second = second.astype(F32) * cap + jnp.sum(
        jnp.where(is_second, before, 0.0), axis=1, keepdims=True
    )
    place = lax.broadcasted_iota(jnp.int32, (1, half * cap), 1)
    ident = place + cap * par
    for k in range(1, half):
        ident = ident + jnp.where(place >= k * cap, cap, 0)
    ident = ident.astype(F32)
    pick[0] = jnp.where(key_first == ident, 1.0, 0.0).astype(BF16)
    pick[1] = jnp.where(key_second == ident, 1.0, 0.0).astype(BF16)

    loads[0].wait()
    chunk = 32

    def norm(i):
        at = pl.ds(pl.multiple_of(i * chunk, chunk), chunk)
        values = tok_v[at, :].astype(F32)
        mean = jnp.mean(values, axis=1, keepdims=True)
        centred = values - mean
        spread = jnp.mean(centred * centred, axis=1, keepdims=True)
        mine = tok_v[at, pl.ds(pl.multiple_of(y * feats, feats), feats)].astype(F32)
        normed_v[at, :] = ((mine - mean) * lax.rsqrt(spread + EPS)).astype(BF16)

    loop(0, tok // chunk, norm)
    picked = lax.dot_general(
        pick[0] + pick[1],
        normed_v[...],
        (((0,), (0,)), ((), ())),
        preferred_element_type=F32,
    )
    dsend[...] = picked.astype(BF16).reshape(dsend.shape)

    @pl.when(c == 0)
    def _():
        xb[y, lax.div(me, 2)] = dsend[lax.div(me, 2)]

    column = jnp.broadcast_to(gain_ref[...], (rows, rows)).T
    for copy in loads[1:]:
        copy.wait()

    def fold(e):
        wsend[e, 0] = (wf[0, e] * column).astype(BF16)
        wsend[e, 1] = (wf[1, e] * column).astype(BF16)
        wsend[e, 2] = wf[2, e].astype(BF16)

    loop(0, F, fold)
    for p in range(3):
        wown[p, me] = wsend[me, p]

    pl.semaphore_wait(barrier, F - 1 + G - 1 + 3)

    def tok_copy(k):
        return pltpu.make_async_remote_copy(
            src_ref=dsend.at[k],
            dst_ref=xb.at[y, lax.div(me, 2)],
            send_sem=tok_s.at[k],
            recv_sem=tok_r.at[lax.div(me, 2)],
            device_id={"fs": 2 * k + par},
            device_id_type=MESH,
        )

    def tok_arrival(k):
        return pltpu.make_async_remote_copy(
            src_ref=dsend.at[k],
            dst_ref=xb.at[y, k],
            send_sem=tok_s.at[k],
            recv_sem=tok_r.at[k],
            device_id={"fs": 2 * k + par},
            device_id_type=MESH,
        )

    def send_tok(m):
        k = lax.rem(lax.div(me, 2) + half // 2 + m, half)

        @pl.when(2 * k + par != me)
        def _():
            tok_copy(k).start()

    loop(0, half, send_tok)

    kinds = (pl.ds(0, 2), pl.ds(2, 1))
    mine = pl.ds(pl.multiple_of(g * share, share), share)

    def z_copy(kind, m):
        to = lax.rem(me + offset(m), F)
        return pltpu.make_async_remote_copy(
            src_ref=wsend.at[to, kinds[kind], mine],
            dst_ref=wown.at[kinds[kind], me, mine],
            send_sem=z_s.at[kind, m],
            recv_sem=z_r.at[kind, m],
            device_id={"fs": to},
            device_id_type=MESH,
        )

    def source(m):
        return lax.rem(me + F - offset(m), F)

    def x_copy(kind, m, n):
        at = wown.at[kinds[kind], source(m), mine]
        return pltpu.make_async_remote_copy(
            src_ref=at,
            dst_ref=at,
            send_sem=x_s.at[kind, n - 1, m],
            recv_sem=x_r.at[kind, n - 1, m],
            device_id={"grp": lax.rem(g + n, G)},
            device_id_type=MESH,
        )

    def d_copy(kind, m, s):
        return pltpu.make_async_remote_copy(
            src_ref=wown.at[kinds[kind], s],
            dst_ref=wpart.at[kinds[kind], s],
            send_sem=d_s.at[kind, m],
            recv_sem=d_r.at[kind, m],
            device_id={"tp": partner},
            device_id_type=MESH,
        )

    def pass_on(kind, m):
        z_copy(kind, m).wait_recv()
        for n in range(1, G):
            x_copy(kind, m, n).start()

    def hand_over(kind, m):
        for n in range(1, G):
            x_copy(kind, m, n).wait_recv()
        d_copy(kind, m, source(m)).start()

    for kind in (0, 1):
        loop(1, F, lambda m, kind=kind: z_copy(kind, m).start())
    for kind in (0, 1):
        d_copy(kind, 0, me).start()

    def ag_copy(i, j, to_right):
        blk = lax.rem(y + Y - i, Y) if to_right else lax.rem(y + i, Y)
        at = xb.at[blk, pl.ds(j * per, per)]
        return pltpu.make_async_remote_copy(
            src_ref=at,
            dst_ref=at,
            send_sem=(agr_s if to_right else agl_s).at[i, j],
            recv_sem=(agr_r if to_right else agl_r).at[i, j],
            device_id={"tp": right if to_right else left},
            device_id_type=MESH,
        )

    for j in range(nsub):
        for k in range(j * per, (j + 1) * per):

            @pl.when(2 * k + par != me)
            def _(k=k):
                tok_arrival(k).wait_recv()

        ag_copy(0, j, True).start()
        ag_copy(0, j, False).start()

    def ag_step(i, both):
        for j in range(nsub):
            ag_copy(i - 1, j, True).wait_recv()
            ag_copy(i, j, True).start()
            ag_copy(i - 1, j, False).wait_recv()
            if both:
                ag_copy(i, j, False).start()

    def forward(i):
        for m in (2 * i - 1, 2 * i):

            @pl.when(m < F)
            def _(m=m):
                pass_on(0, m)

    def settle(i):
        for m in (2 * i - 1, 2 * i):

            @pl.when(m < F)
            def _(m=m):
                hand_over(0, m)

    ag_step(1, 1 < left_steps)
    forward(1)

    def middle(i):
        ag_step(i, True)
        forward(i)
        settle(i - 1)

    loop(2, left_steps, middle)
    for i in range(max(2, left_steps), right_steps):
        ag_step(i, i < left_steps)
        forward(i)
        settle(i - 1)
    for j in range(nsub):
        ag_copy(right_steps - 1, j, True).wait_recv()
    settle(right_steps - 1)
    rest = min(F, 2 * right_steps - 1)
    loop(rest, F, lambda m: pass_on(0, m))
    loop(1, F // 2, lambda m: pass_on(1, m))
    loop(rest, F, lambda m: hand_over(0, m))
    loop(1, F // 2, lambda m: hand_over(1, m))
    loop(0, F, lambda m: d_copy(0, m, me).wait_recv())
    store_g = pltpu.make_async_copy(wown.at[0], go_hbm.at[0], store_sem.at[0])
    store_u = pltpu.make_async_copy(wown.at[1], uo_hbm.at[0], store_sem.at[1])
    store_g.start()
    store_u.start()

    acc_g[...] = jnp.zeros_like(acc_g)
    acc_u[...] = jnp.zeros_like(acc_u)
    area = half * cap

    def contract(m):
        lhs = jnp.concatenate(
            [xb[2 * m].reshape(area, feats), xb[2 * m + 1].reshape(area, feats)], axis=1
        )

        def rhs(p):
            top = jnp.concatenate([wown[p, 2 * m], wpart[p, 2 * m]], axis=1)
            low = jnp.concatenate([wown[p, 2 * m + 1], wpart[p, 2 * m + 1]], axis=1)
            return jnp.concatenate([top, low], axis=0)

        acc_g[...] += jnp.dot(lhs, rhs(0), preferred_element_type=F32)
        acc_u[...] += jnp.dot(lhs, rhs(1), preferred_element_type=F32)

    loop(0, Y // 2, contract)

    def activate(k):
        at = pl.ds(pl.multiple_of(k * cap, cap), cap)
        v = acc_g[at, :]
        hid[at, :] = (v / (1.0 + jnp.exp(-v)) * acc_u[at, :]).astype(BF16)

    loop(0, half, activate)

    loop(F // 2, F, lambda m: pass_on(1, m))
    loop(F // 2, F, lambda m: hand_over(1, m))
    loop(0, F, lambda m: d_copy(1, m, me).wait_recv())
    store_d = pltpu.make_async_copy(wown.at[2], do_hbm.at[0], store_sem.at[2])
    store_d.start()

    def product(d):
        block = jnp.concatenate([wown[2, d], wpart[2, d]], axis=1)
        return lax.dot_general(
            hid[...], block, (((1,), (1,)), ((), ())), preferred_element_type=F32
        )

    sub = per * cap

    def rs_copy(i, j, to_right):
        return pltpu.make_async_remote_copy(
            src_ref=(rs_rsend if to_right else rs_lsend).at[i, j],
            dst_ref=(rs_rrecv if to_right else rs_lrecv).at[i, j],
            send_sem=(rsr_s if to_right else rsl_s).at[i, j],
            recv_sem=(rsr_r if to_right else rsl_r).at[i, j],
            device_id={"tp": right if to_right else left},
            device_id_type=MESH,
        )

    def right_chunk(i):
        return lax.rem(y + right_steps + Y - i, Y)

    def left_chunk(i):
        return lax.rem(y + Y - left_steps + i, Y)

    part_r[...] = product(right_chunk(0))
    for j in range(nsub):
        rs_rsend[0, j] = part_r[pl.ds(j * sub, sub), :].astype(BF16)
        rs_copy(0, j, True).start()
    part_l[...] = product(left_chunk(0))
    for j in range(nsub):
        rs_lsend[0, j] = part_l[pl.ds(j * sub, sub), :].astype(BF16)
        rs_copy(0, j, False).start()

    def rs_step(i, both):
        part_r[...] = product(right_chunk(i))
        if both:
            part_l[...] = product(left_chunk(i))
        for j in range(nsub):
            at = pl.ds(j * sub, sub)
            rs_copy(i - 1, j, True).wait_recv()
            rs_rsend[i, j] = (rs_rrecv[i - 1, j].astype(F32) + part_r[at, :]).astype(BF16)
            rs_copy(i, j, True).start()
            if both:
                rs_copy(i - 1, j, False).wait_recv()
                rs_lsend[i, j] = (rs_lrecv[i - 1, j].astype(F32) + part_l[at, :]).astype(BF16)
                rs_copy(i, j, False).start()

    loop(1, left_steps, lambda i: rs_step(i, True))
    for i in range(max(1, left_steps), right_steps):
        rs_step(i, False)

    def ret_copy(k):
        return pltpu.make_async_remote_copy(
            src_ref=ret_send.at[k],
            dst_ref=ret_recv.at[lax.div(me, 2)],
            send_sem=ret_s.at[k],
            recv_sem=ret_r.at[lax.div(me, 2)],
            device_id={"fs": 2 * k + par},
            device_id_type=MESH,
        )

    def ret_arrival(k):
        return pltpu.make_async_remote_copy(
            src_ref=ret_send.at[k],
            dst_ref=ret_recv.at[k],
            send_sem=ret_s.at[k],
            recv_sem=ret_r.at[k],
            device_id={"fs": 2 * k + par},
            device_id_type=MESH,
        )

    part_r[...] = product(y)
    for j in range(nsub):
        rs_copy(left_steps - 1, j, False).wait_recv()
        rs_copy(right_steps - 1, j, True).wait_recv()
        total = (
            part_r[pl.ds(j * sub, sub), :]
            + rs_rrecv[right_steps - 1, j].astype(F32)
            + rs_lrecv[left_steps - 1, j].astype(F32)
        ).astype(BF16)
        ret_send[pl.ds(j * per, per)] = total.reshape(per, cap, feats)
        for k in range(j * per, (j + 1) * per):

            @pl.when(2 * k + par != me)
            def _(k=k):
                ret_copy(k).start()

    @pl.when(c == 0)
    def _():
        ret_recv[lax.div(me, 2)] = ret_send[lax.div(me, 2)]

    diff = logits_ref[:, 0:1] - logits_ref[:, 1:2]
    share_first = 1.0 / (1.0 + jnp.exp(-diff))
    share_second = 1.0 / (1.0 + jnp.exp(diff))

    for k in range(half):

        @pl.when(2 * k + par != me)
        def _(k=k):
            ret_arrival(k).wait_recv()

    returned = ret_recv[...].reshape(area, feats)
    mix_own[...] = share_first * jnp.dot(
        pick[0], returned, preferred_element_type=F32
    ) + share_second * jnp.dot(pick[1], returned, preferred_element_type=F32)
    swap = pltpu.make_async_remote_copy(
        src_ref=mix_own,
        dst_ref=mix_other,
        send_sem=mix_s,
        recv_sem=mix_r,
        device_id={"tp": partner},
        device_id_type=MESH,
    )
    swap.start()
    swap.wait_recv()
    both = mix_own[...] + mix_other[...]
    width = mix_ref.shape[1]
    mix_ref[...] = jnp.where(c == 0, both[:, :width], both[:, width:]).astype(BF16)

    swap.wait_send()
    for copy in (store_g, store_u, store_d):
        copy.wait()

    def drain_tok(k):
        @pl.when(2 * k + par != me)
        def _():
            tok_copy(k).wait_send()
            ret_copy(k).wait_send()

    loop(0, half, drain_tok)
    for kind in (0, 1):

        def drain(m, kind=kind):
            z_copy(kind, m).wait_send()
            for n in range(1, G):
                x_copy(kind, m, n).wait_send()

        loop(1, F, drain)
        loop(0, F, lambda m, kind=kind: d_copy(kind, m, me).wait_send())

    def drain_ring(i):
        for j in range(nsub):
            ag_copy(i, j, True).wait_send()
            rs_copy(i, j, True).wait_send()

    def drain_ring_left(i):
        for j in range(nsub):
            ag_copy(i, j, False).wait_send()
            rs_copy(i, j, False).wait_send()

    loop(0, right_steps, drain_ring)
    loop(0, left_steps, drain_ring_left)


def solution(mesh):
    G, F, Y = mesh.shape["grp"], mesh.shape["fs"], mesh.shape["tp"] // 2

    def on_device(tokens, routes, route_logits, gain, w_gate, w_up, w_down):
        experts, rows, cols = w_gate.shape
        tok, width = tokens.shape
        cap = 3 * tok // experts
        half = F // 2
        nsub = min(4, half)
        feats = width // Y
        area = half * cap
        rs, ls = Y // 2, Y // 2 - 1
        any_spec = pl.BlockSpec(memory_space=pl.ANY)
        vmem = pl.BlockSpec(memory_space=pltpu.VMEM)
        dma = pltpu.SemaphoreType.DMA
        out = jax.ShapeDtypeStruct((1, F, rows, cols), BF16)
        gate_out, up_out, down_out, mixed = pl.pallas_call(
            functools.partial(kernel, (G, F, Y, cap, nsub)),
            out_shape=(out, out, out, jax.ShapeDtypeStruct((tok, feats // 2), BF16)),
            in_specs=[any_spec, vmem, vmem, vmem, any_spec, any_spec, any_spec],
            out_specs=(any_spec, any_spec, any_spec, vmem),
            scratch_shapes=[
                pltpu.VMEM((tok, width), BF16),
                pltpu.VMEM((tok, feats), BF16),
                pltpu.VMEM((3, F, rows, cols), F32),
                pltpu.VMEM((F, 3, rows, cols), BF16),
                pltpu.VMEM((3, F, rows, cols), BF16),
                pltpu.VMEM((3, F, rows, cols), BF16),
                pltpu.VMEM((Y, half, cap, feats), BF16),
                pltpu.VMEM((half, cap, feats), BF16),
                pltpu.VMEM((2, tok, area), BF16),
                pltpu.VMEM((area, 2 * cols), BF16),
                pltpu.VMEM((area, 2 * cols), F32),
                pltpu.VMEM((area, 2 * cols), F32),
                pltpu.VMEM((area, feats), F32),
                pltpu.VMEM((area, feats), F32),
                pltpu.VMEM((rs, nsub, area // nsub, feats), BF16),
                pltpu.VMEM((ls, nsub, area // nsub, feats), BF16),
                pltpu.VMEM((rs, nsub, area // nsub, feats), BF16),
                pltpu.VMEM((ls, nsub, area // nsub, feats), BF16),
                pltpu.VMEM((half, cap, feats), BF16),
                pltpu.VMEM((half, cap, feats), BF16),
                pltpu.VMEM((tok, feats), F32),
                pltpu.VMEM((tok, feats), F32),
                dma((4,)),
                dma((3,)),
                dma((half,)),
                dma((half,)),
                dma((2, F)),
                dma((2, F)),
                dma((2, max(G - 1, 1), F)),
                dma((2, max(G - 1, 1), F)),
                dma((2, F)),
                dma((2, F)),
                dma((rs, nsub)),
                dma((rs, nsub)),
                dma((ls, nsub)),
                dma((ls, nsub)),
                dma((rs, nsub)),
                dma((rs, nsub)),
                dma((ls, nsub)),
                dma((ls, nsub)),
                dma((half,)),
                dma((half,)),
                dma,
                dma,
            ],
            compiler_params=pltpu.CompilerParams(collective_id=0, has_side_effects=True),
        )(tokens, routes, route_logits, gain.reshape(1, rows), w_gate, w_up, w_down)
        weights = tuple(w.reshape(1, F * rows, cols) for w in (gate_out, up_out, down_out))
        return (*weights, mixed)

    in_specs = (
        P(("grp", "fs"), None),
        P(("grp", "fs"), None),
        P(("grp", "fs"), None),
        P("fs"),
        P(None, "fs", "tp"),
        P(None, "fs", "tp"),
        P(None, "fs", "tp"),
    )
    out_specs = (
        P(("grp", "fs"), None, "tp"),
        P(("grp", "fs"), None, "tp"),
        P(("grp", "fs"), None, "tp"),
        P(("grp", "fs"), "tp"),
    )
    return jax.shard_map(
        on_device, mesh=mesh, in_specs=in_specs, out_specs=out_specs, check_vma=False
    )
```

```python
import functools

import jax
import jax.numpy as jnp
from jax import lax
from jax.experimental import pallas as pl
from jax.experimental.pallas import tpu as pltpu
from jax.sharding import PartitionSpec as P

EPS = 1e-06
MESH = pl.DeviceIdType.MESH
F32 = jnp.float32
BF16 = jnp.bfloat16


def loop(lo, hi, body):
    def step(i, carry):
        body(i)
        return carry

    lax.fori_loop(lo, hi, step, 0)


def kernel(
    dims,
    tokens_hbm,
    routes_ref,
    logits_ref,
    gain_ref,
    wg_hbm,
    wu_hbm,
    wd_hbm,
    go_hbm,
    uo_hbm,
    do_hbm,
    mix_ref,
    tok_v,
    normed_v,
    wf,
    wsend,
    wown,
    wpart,
    xb,
    dsend,
    pick,
    hid,
    acc_g,
    acc_u,
    part_r,
    part_l,
    rs_rsend,
    rs_lsend,
    rs_rrecv,
    rs_lrecv,
    ret_send,
    ret_recv,
    share_tab,
    mix_own,
    mix_other,
    load_sem,
    store_sem,
    tok_s,
    tok_r,
    z_s,
    z_r,
    x_s,
    x_r,
    d_s,
    d_r,
    agr_s,
    agr_r,
    agl_s,
    agl_r,
    rsr_s,
    rsr_r,
    rsl_s,
    rsl_r,
    ret_s,
    ret_r,
    mix_s,
    mix_r,
):
    G, F, Y, cap, nsub = dims
    half = F // 2
    per = half // nsub
    right_steps, left_steps = Y // 2, Y // 2 - 1
    rows = wsend.shape[2]
    share = rows // G
    feats = xb.shape[3]

    g = lax.axis_index("grp")
    me = lax.axis_index("fs")
    t = lax.axis_index("tp")
    y = lax.div(t, 2)
    c = lax.rem(t, 2)
    partner = t + 1 - 2 * c
    right = lax.rem(y + 1, Y) * 2 + c
    left = lax.rem(y + Y - 1, Y) * 2 + c
    par = lax.rem(me + c, 2)

    def taken(sem, refs):
        pltpu.make_async_copy(refs, refs, sem).wait()

    def offset(m):
        step = lax.div(m + 1, 2)
        odd = lax.rem(m, 2)
        return odd * step + (1 - odd) * (F - step)

    barrier = pltpu.get_barrier_semaphore()

    def greet(m):
        pl.semaphore_signal(
            barrier, inc=1, device_id={"fs": lax.rem(me + m, F)}, device_id_type=MESH
        )

    loop(1, F, greet)
    for m in range(1, G):
        pl.semaphore_signal(
            barrier, inc=1, device_id={"grp": lax.rem(g + m, G)}, device_id_type=MESH
        )
    for other in (partner, left, right):
        pl.semaphore_signal(barrier, inc=1, device_id={"tp": other}, device_id_type=MESH)

    loads = [pltpu.make_async_copy(tokens_hbm, tok_v, load_sem.at[0])]
    for p, ref in enumerate((wg_hbm, wu_hbm, wd_hbm)):
        loads.append(pltpu.make_async_copy(ref, wf.at[p], load_sem.at[p + 1]))
    for copy in loads:
        copy.start()

    tok = tok_v.shape[0]
    lanes = 128
    experts = lax.broadcasted_iota(jnp.int32, (tok, lanes), 1).astype(F32)
    line = lax.broadcasted_iota(jnp.int32, (8, tok), 0)
    table = jnp.where(
        line == 0,
        routes_ref[0:1, :].astype(F32),
        jnp.where(
            line == 1,
            routes_ref[1:2, :].astype(F32),
            jnp.where(line == 2, logits_ref[0:1, :], logits_ref[1:2, :]),
        ),
    ).T
    first = table[:, 0:1]
    second = table[:, 1:2]
    is_first = first == experts
    is_second = second == experts
    marked = jnp.where(is_first | is_second, 1.0, 0.0).astype(BF16)
    earlier = jnp.where(
        lax.broadcasted_iota(jnp.int32, (tok, tok), 1)
        < lax.broadcasted_iota(jnp.int32, (tok, tok), 0),
        1.0,
        0.0,
    ).astype(BF16)
    before = jnp.dot(earlier, marked, preferred_element_type=F32)
    key_first = first * cap + jnp.sum(
        jnp.where(is_first, before, 0.0), axis=1, keepdims=True
    )
    key_second = second * cap + jnp.sum(
        jnp.where(is_second, before, 0.0), axis=1, keepdims=True
    )
    place = lax.broadcasted_iota(jnp.int32, (1, half * cap), 1)
    ident = place + cap * par
    for k in range(1, half):
        ident = ident + jnp.where(place >= k * cap, cap, 0)
    ident = ident.astype(F32)
    pick[0] = jnp.where(key_first == ident, 1.0, 0.0).astype(BF16)
    pick[1] = jnp.where(key_second == ident, 1.0, 0.0).astype(BF16)

    diff = table[:, 2:3] - table[:, 3:4]
    share_tab[0] = jnp.broadcast_to(1.0 / (1.0 + jnp.exp(-diff)), (tok, lanes))
    share_tab[1] = jnp.broadcast_to(1.0 / (1.0 + jnp.exp(diff)), (tok, lanes))

    loads[0].wait()
    chunk = 32

    def norm(i):
        at = pl.ds(pl.multiple_of(i * chunk, chunk), chunk)
        values = tok_v[at, :].astype(F32)
        mean = jnp.mean(values, axis=1, keepdims=True)
        centred = values - mean
        spread = jnp.mean(centred * centred, axis=1, keepdims=True)
        mine = tok_v[at, pl.ds(pl.multiple_of(y * feats, feats), feats)].astype(F32)
        normed_v[at, :] = ((mine - mean) * lax.rsqrt(spread + EPS)).astype(BF16)

    loop(0, tok // chunk, norm)
    picked = lax.dot_general(
        pick[0] + pick[1],
        normed_v[...],
        (((0,), (0,)), ((), ())),
        preferred_element_type=F32,
    )
    dsend[...] = picked.astype(BF16).reshape(dsend.shape)

    @pl.when(c == 0)
    def _():
        xb[y, lax.div(me, 2)] = dsend[lax.div(me, 2)]

    column = jnp.broadcast_to(gain_ref[...], (rows, rows)).T
    for copy in loads[1:]:
        copy.wait()

    def fold(e):
        wsend[e, 0] = (wf[0, e] * column).astype(BF16)
        wsend[e, 1] = (wf[1, e] * column).astype(BF16)
        wsend[e, 2] = wf[2, e].astype(BF16)

    loop(0, F, fold)
    for p in range(3):
        wown[p, me] = wsend[me, p]

    pl.semaphore_wait(barrier, F - 1 + G - 1 + 3)

    def tok_copy(k):
        return pltpu.make_async_remote_copy(
            src_ref=dsend.at[k],
            dst_ref=xb.at[y, lax.div(me, 2)],
            send_sem=tok_s,
            recv_sem=tok_r.at[lax.div(me, 2)],
            device_id={"fs": 2 * k + par},
            device_id_type=MESH,
        )

    def tok_arrival(k):
        return pltpu.make_async_remote_copy(
            src_ref=dsend.at[k],
            dst_ref=xb.at[y, k],
            send_sem=tok_s,
            recv_sem=tok_r.at[k],
            device_id={"fs": 2 * k + par},
            device_id_type=MESH,
        )

    kinds = (pl.ds(0, 2), pl.ds(2, 1))
    mine = pl.ds(pl.multiple_of(g * share, share), share)

    def z_copy(kind, to, source):
        return pltpu.make_async_remote_copy(
            src_ref=wsend.at[to, kinds[kind], mine],
            dst_ref=wown.at[kinds[kind], source, mine],
            send_sem=z_s,
            recv_sem=z_r.at[kind, source],
            device_id={"fs": to},
            device_id_type=MESH,
        )

    def x_copy(kind, s, n):
        at = wown.at[kinds[kind], s, mine]
        return pltpu.make_async_remote_copy(
            src_ref=at,
            dst_ref=at,
            send_sem=x_s.at[n - 1],
            recv_sem=x_r.at[kind, n - 1, s],
            device_id={"grp": lax.rem(g + n, G)},
            device_id_type=MESH,
        )

    def d_copy(kind, s):
        return pltpu.make_async_remote_copy(
            src_ref=wown.at[kinds[kind], s],
            dst_ref=wpart.at[kinds[kind], s],
            send_sem=d_s,
            recv_sem=d_r.at[kind * (s + 1)],
            device_id={"tp": partner},
            device_id_type=MESH,
        )

    def pass_on(kind, s):
        z_copy(kind, s, s).wait_recv()
        for n in range(1, G):
            x_copy(kind, s, n).start()

    def hand_over(kind, s):
        for n in range(1, G):
            x_copy(kind, s, n).wait_recv()
        d_copy(kind, s).start()

    def send_tok(k):
        @pl.when(lax.rem(k, 2) == par)
        def _():
            tok_copy(lax.div(k, 2)).start()

    def send_tok(m):
        k = lax.rem(lax.div(me, 2) + half // 2 + m, half)

        @pl.when(2 * k + par != me)
        def _():
            tok_copy(k).start()

    loop(0, half, send_tok)
    def send_weights(kind):
        loop(1, F, lambda m: z_copy(kind, lax.rem(me + offset(m), F), me).start())

    ahead = lax.rem(me + F - y, F)
    soon = (ahead >= F // 4 + 1) & (ahead <= F - F // 4)
    send_weights(0)

    @pl.when(soon)
    def _():
        send_weights(1)

    for kind in (0, 1):
        d_copy(kind, me).start()

    def source(m):
        return lax.rem(me + F - offset(m), F)

    def ag_copy(i, j, to_right):
        blk = lax.rem(y + Y - i, Y) if to_right else lax.rem(y + i, Y)
        at = xb.at[blk, pl.ds(j * per, per)]
        return pltpu.make_async_remote_copy(
            src_ref=at,
            dst_ref=at,
            send_sem=agr_s if to_right else agl_s,
            recv_sem=(agr_r if to_right else agl_r).at[i, j],
            device_id={"tp": right if to_right else left},
            device_id_type=MESH,
        )

    for j in range(nsub):
        for k in range(j * per, (j + 1) * per):

            @pl.when(2 * k + par != me)
            def _(k=k):
                tok_arrival(k).wait_recv()

        ag_copy(0, j, True).start()
        ag_copy(0, j, False).start()

    def ag_step(i, both):
        for j in range(nsub):
            ag_copy(i - 1, j, True).wait_recv()
            ag_copy(i, j, True).start()
            ag_copy(i - 1, j, False).wait_recv()
            if both:
                ag_copy(i, j, False).start()

    def forward(act, kind, i):
        for m in (2 * i - 1, 2 * i):

            @pl.when((m > 0) & (m < F))
            def _(m=m):
                act(kind, source(m))

    def tend(i):
        forward(pass_on, 0, i)
        forward(hand_over, 0, i - 1)

    def middle(i):
        ag_step(i, True)
        tend(i)

    loop(1, left_steps, middle)
    for i in range(left_steps, right_steps):
        ag_step(i, i < left_steps)
        tend(i)

    @pl.when(jnp.logical_not(soon))
    def _():
        send_weights(1)

    loop(right_steps, F // 2 + 2, tend)
    taken(d_r.at[0], wpart.at[kinds[0]])
    store_g = pltpu.make_async_copy(wown.at[0], go_hbm.at[0], store_sem.at[0])
    store_u = pltpu.make_async_copy(wown.at[1], uo_hbm.at[0], store_sem.at[1])
    store_g.start()
    store_u.start()

    acc_g[...] = jnp.zeros_like(acc_g)
    acc_u[...] = jnp.zeros_like(acc_u)
    area = half * cap

    def contract(a, b):
        lhs = jnp.concatenate(
            [xb[a].reshape(area, feats), xb[b].reshape(area, feats)], axis=1
        )

        def rhs(p):
            top = jnp.concatenate([wown[p, a], wpart[p, a]], axis=1)
            low = jnp.concatenate([wown[p, b], wpart[p, b]], axis=1)
            return jnp.concatenate([top, low], axis=0)

        acc_g[...] += jnp.dot(lhs, rhs(0), preferred_element_type=F32)
        acc_u[...] += jnp.dot(lhs, rhs(1), preferred_element_type=F32)

    loop(1, left_steps + 1, lambda i: contract(lax.rem(y + Y - i, Y), lax.rem(y + i, Y)))
    for j in range(nsub):
        ag_copy(right_steps - 1, j, True).wait_recv()
    contract(y, lax.rem(y + right_steps, Y))

    def activate(k):
        at = pl.ds(pl.multiple_of(k * cap, cap), cap)
        v = acc_g[at, :]
        hid[at, :] = (v / (1.0 + jnp.exp(-v)) * acc_u[at, :]).astype(BF16)

    loop(0, half, activate)

    def product(d):
        block = jnp.concatenate([wown[2, d], wpart[2, d]], axis=1)
        return lax.dot_general(
            hid[...], block, (((1,), (1,)), ((), ())), preferred_element_type=F32
        )

    sub = per * cap

    def rs_copy(i, j, to_right):
        return pltpu.make_async_remote_copy(
            src_ref=(rs_rsend if to_right else rs_lsend).at[i, j],
            dst_ref=(rs_rrecv if to_right else rs_lrecv).at[i, j],
            send_sem=rsr_s if to_right else rsl_s,
            recv_sem=(rsr_r if to_right else rsl_r).at[i, j],
            device_id={"tp": right if to_right else left},
            device_id_type=MESH,
        )

    def right_chunk(i):
        return lax.rem(y + right_steps + Y - i, Y)

    def left_chunk(i):
        return lax.rem(y + Y - left_steps + i, Y)

    def chunk_of(n):
        i = lax.div(n, 2)
        odd = lax.rem(n, 2)
        return lax.rem(y + Y + (1 - odd) * (right_steps - i) + odd * (i - left_steps), Y)

    def down_block(act, n):
        s = chunk_of(n)

        @pl.when((n < F) & (s != me))
        def _():
            act(1, s)

    def down_ready(i, both=True):
        for n in (2 * i + 4, 2 * i + 5):
            down_block(pass_on, n)
        for n in (2 * i + 2, 2 * i + 3):
            down_block(hand_over, n)
        d_copy(1, chunk_of(2 * i)).wait_recv()
        if both:
            d_copy(1, chunk_of(2 * i + 1)).wait_recv()

    for n in range(4):
        down_block(pass_on, n)
    for n in range(2):
        down_block(hand_over, n)
    down_ready(0)
    part_r[...] = product(right_chunk(0))
    for j in range(nsub):
        rs_rsend[0, j] = part_r[pl.ds(j * sub, sub), :].astype(BF16)
        rs_copy(0, j, True).start()
    part_l[...] = product(left_chunk(0))
    for j in range(nsub):
        rs_lsend[0, j] = part_l[pl.ds(j * sub, sub), :].astype(BF16)
        rs_copy(0, j, False).start()

    def rs_step(i, both):
        down_ready(i)
        part_r[...] = product(right_chunk(i))
        if both:
            part_l[...] = product(left_chunk(i))
        for j in range(nsub):
            at = pl.ds(j * sub, sub)
            rs_copy(i - 1, j, True).wait_recv()
            rs_rsend[i, j] = (rs_rrecv[i - 1, j].astype(F32) + part_r[at, :]).astype(BF16)
            rs_copy(i, j, True).start()
            if both:
                rs_copy(i - 1, j, False).wait_recv()
                rs_lsend[i, j] = (rs_lrecv[i - 1, j].astype(F32) + part_l[at, :]).astype(BF16)
                rs_copy(i, j, False).start()

    loop(1, left_steps, lambda i: rs_step(i, True))
    for i in range(max(1, left_steps), right_steps):
        rs_step(i, False)

    def ret_copy(k):
        return pltpu.make_async_remote_copy(
            src_ref=ret_send.at[k],
            dst_ref=ret_recv.at[lax.div(me, 2)],
            send_sem=ret_s,
            recv_sem=ret_r,
            device_id={"fs": 2 * k + par},
            device_id_type=MESH,
        )

    store_d = pltpu.make_async_copy(wown.at[2], do_hbm.at[0], store_sem.at[2])
    store_d.start()
    part_r[...] = product(y)
    for j in range(nsub):
        rs_copy(left_steps - 1, j, False).wait_recv()
        rs_copy(right_steps - 1, j, True).wait_recv()
        total = (
            part_r[pl.ds(j * sub, sub), :]
            + rs_rrecv[right_steps - 1, j].astype(F32)
            + rs_lrecv[left_steps - 1, j].astype(F32)
        ).astype(BF16)
        ret_send[pl.ds(j * per, per)] = total.reshape(per, cap, feats)
        for k in range(j * per, (j + 1) * per):

            @pl.when(2 * k + par != me)
            def _(k=k):
                ret_copy(k).start()

    @pl.when(c == 0)
    def _():
        ret_recv[lax.div(me, 2)] = ret_send[lax.div(me, 2)]

    def all_but_own(sem, ref):
        @pl.when(c == 0)
        def _():
            taken(sem, ref.at[pl.ds(0, half - 1)])

        @pl.when(c == 1)
        def _():
            taken(sem, ref)

    all_but_own(ret_r, ret_recv)
    returned = ret_recv[...].reshape(area, feats)
    mix_own[...] = share_tab[0] * jnp.dot(
        pick[0], returned, preferred_element_type=F32
    ) + share_tab[1] * jnp.dot(pick[1], returned, preferred_element_type=F32)
    swap = pltpu.make_async_remote_copy(
        src_ref=mix_own,
        dst_ref=mix_other,
        send_sem=mix_s,
        recv_sem=mix_r,
        device_id={"tp": partner},
        device_id_type=MESH,
    )
    swap.start()
    swap.wait_recv()
    both = (mix_own[...] + mix_other[...]).T
    width = mix_ref.shape[0]
    mix_ref[...] = jnp.where(c == 0, both[:width, :], both[width:, :]).astype(BF16)

    swap.wait_send()
    for copy in (store_g, store_u, store_d):
        copy.wait()

    all_but_own(tok_s, dsend)
    all_but_own(ret_s, ret_send)
    taken(z_s, wsend.at[pl.ds(0, F - 1), :, mine])
    for n in range(1, G):
        taken(x_s.at[n - 1], wown.at[:, pl.ds(0, F - 1), mine])
    taken(d_s, wown)
    taken(agr_s, xb.at[pl.ds(0, right_steps)])
    taken(agl_s, xb.at[pl.ds(0, left_steps)])
    taken(rsr_s, rs_rsend)
    taken(rsl_s, rs_lsend)


def hand_in(n, *refs):
    sources, results, holds, sems = refs[:n], refs[n : 2 * n], refs[2 * n : 3 * n], refs[3 * n]
    ins = [pltpu.make_async_copy(sources[i], holds[i], sems.at[0, i]) for i in range(n)]
    outs = [pltpu.make_async_copy(holds[i], results[i], sems.at[1, i]) for i in range(n)]
    for copy in ins:
        copy.start()
    for i in range(n):
        ins[i].wait()
        outs[i].start()
    for copy in outs:
        copy.wait()


def solution(mesh):
    G, F, Y = mesh.shape["grp"], mesh.shape["fs"], mesh.shape["tp"] // 2

    def on_device(tokens, routes, route_logits, gain, w_gate, w_up, w_down):
        experts, rows, cols = w_gate.shape
        tok, width = tokens.shape
        cap = 3 * tok // experts
        half = F // 2
        nsub = min(4, half)
        feats = width // Y
        area = half * cap
        rs, ls = Y // 2, Y // 2 - 1
        any_spec = pl.BlockSpec(memory_space=pl.ANY)
        vmem = pl.BlockSpec(memory_space=pltpu.VMEM)
        dma = pltpu.SemaphoreType.DMA
        out = jax.ShapeDtypeStruct((1, F, rows, cols), BF16)
        made = pl.pallas_call(
            functools.partial(kernel, (G, F, Y, cap, nsub)),
            out_shape=(out, out, out, jax.ShapeDtypeStruct((feats // 2, tok), BF16)),
            in_specs=[any_spec, vmem, vmem, vmem, any_spec, any_spec, any_spec],
            out_specs=(any_spec, any_spec, any_spec, vmem),
            scratch_shapes=[
                pltpu.VMEM((tok, width), BF16),
                pltpu.VMEM((tok, feats), BF16),
                pltpu.VMEM((3, F, rows, cols), F32),
                pltpu.VMEM((F, 3, rows, cols), BF16),
                pltpu.VMEM((3, F, rows, cols), BF16),
                pltpu.VMEM((3, F, rows, cols), BF16),
                pltpu.VMEM((Y, half, cap, feats), BF16),
                pltpu.VMEM((half, cap, feats), BF16),
                pltpu.VMEM((2, tok, area), BF16),
                pltpu.VMEM((area, 2 * cols), BF16),
                pltpu.VMEM((area, 2 * cols), F32),
                pltpu.VMEM((area, 2 * cols), F32),
                pltpu.VMEM((area, feats), F32),
                pltpu.VMEM((area, feats), F32),
                pltpu.VMEM((rs, nsub, area // nsub, feats), BF16),
                pltpu.VMEM((ls, nsub, area // nsub, feats), BF16),
                pltpu.VMEM((rs, nsub, area // nsub, feats), BF16),
                pltpu.VMEM((ls, nsub, area // nsub, feats), BF16),
                pltpu.VMEM((half, cap, feats), BF16),
                pltpu.VMEM((half, cap, feats), BF16),
                pltpu.VMEM((2, tok, feats), F32),
                pltpu.VMEM((tok, feats), F32),
                pltpu.VMEM((tok, feats), F32),
                dma((4,)),
                dma((3,)),
                dma,
                dma((half,)),
                dma,
                dma((2, F)),
                dma((max(G - 1, 1),)),
                dma((2, max(G - 1, 1), F)),
                dma,
                dma((F + 1,)),
                dma,
                dma((rs, nsub)),
                dma,
                dma((ls, nsub)),
                dma,
                dma((rs, nsub)),
                dma,
                dma((ls, nsub)),
                dma,
                dma,
                dma,
                dma,
            ],
            compiler_params=pltpu.CompilerParams(collective_id=0, has_side_effects=True),
        )(tokens, routes.T, route_logits.T, gain.reshape(1, rows), w_gate, w_up, w_down)
        gate_out, up_out, down_out, mixed = pl.pallas_call(
            functools.partial(hand_in, 4),
            out_shape=[jax.ShapeDtypeStruct(a.shape, a.dtype) for a in made],
            in_specs=[any_spec] * 4,
            out_specs=[any_spec] * 4,
            scratch_shapes=[pltpu.VMEM(a.shape, a.dtype) for a in made] + [dma((2, 4))],
        )(*made)
        weights = tuple(w.reshape(1, F * rows, cols) for w in (gate_out, up_out, down_out))
        return (*weights, mixed.T)

    in_specs = (
        P(("grp", "fs"), None),
        P(("grp", "fs"), None),
        P(("grp", "fs"), None),
        P("fs"),
        P(None, "fs", "tp"),
        P(None, "fs", "tp"),
        P(None, "fs", "tp"),
    )
    out_specs = (
        P(("grp", "fs"), None, "tp"),
        P(("grp", "fs"), None, "tp"),
        P(("grp", "fs"), None, "tp"),
        P(("grp", "fs"), "tp"),
    )
    return jax.shard_map(
        on_device, mesh=mesh, in_specs=in_specs, out_specs=out_specs, check_vma=False
    )
```

```python
import functools

import jax
import jax.numpy as jnp
from jax import lax
from jax.experimental import pallas as pl
from jax.experimental.pallas import tpu as pltpu
from jax.sharding import PartitionSpec as P

EPS = 1e-06
MESH = pl.DeviceIdType.MESH
F32 = jnp.float32
BF16 = jnp.bfloat16


def loop(lo, hi, body):
    def step(i, carry):
        body(i)
        return carry

    lax.fori_loop(lo, hi, step, 0)


def kernel(
    dims,
    tokens_hbm,
    routes_ref,
    logits_ref,
    gain_ref,
    wg_hbm,
    wu_hbm,
    wd_hbm,
    go_hbm,
    uo_hbm,
    do_hbm,
    mix_ref,
    tok_v,
    normed_v,
    wf,
    wsend,
    wown,
    wpart,
    xb,
    dsend,
    pick,
    hid,
    acc_g,
    acc_u,
    part_r,
    part_l,
    rs_rsend,
    rs_lsend,
    rs_rrecv,
    rs_lrecv,
    near_send,
    near_recv,
    ret_send,
    ret_recv,
    key_tab,
    share_tab,
    mix_own,
    mix_other,
    load_sem,
    store_sem,
    tok_s,
    tok_r,
    z_s,
    z_r,
    x_s,
    x_r,
    d_s,
    d_r,
    agr_s,
    agr_r,
    agl_s,
    agl_r,
    near_s,
    near_r,
    rsr_s,
    rsr_r,
    rsl_s,
    rsl_r,
    ret_s,
    ret_r,
    mix_s,
    mix_r,
):
    G, F, Y, cap, nsub, nsum = dims
    half = F // 2
    per = half // nsub
    sum_per = half // nsum
    right_steps, left_steps = Y // 2, Y // 2 - 1
    rows = wsend.shape[2]
    share = rows // G
    feats = xb.shape[3]

    g = lax.axis_index("grp")
    me = lax.axis_index("fs")
    t = lax.axis_index("tp")
    y = lax.div(t, 2)
    c = lax.rem(t, 2)
    partner = t + 1 - 2 * c
    right = lax.rem(y + 1, Y) * 2 + c
    left = lax.rem(y + Y - 1, Y) * 2 + c
    par = lax.rem(me + c, 2)

    def taken(sem, refs):
        pltpu.make_async_copy(refs, refs, sem).wait()

    def offset(m):
        step = lax.div(m + 1, 2)
        odd = lax.rem(m, 2)
        return odd * step + (1 - odd) * (F - step)

    barrier = pltpu.get_barrier_semaphore()

    def greet(m):
        pl.semaphore_signal(
            barrier, inc=1, device_id={"fs": lax.rem(me + m, F)}, device_id_type=MESH
        )

    loop(1, F, greet)
    for m in range(1, G):
        pl.semaphore_signal(
            barrier, inc=1, device_id={"grp": lax.rem(g + m, G)}, device_id_type=MESH
        )
    for other in (partner, left, right):
        pl.semaphore_signal(barrier, inc=1, device_id={"tp": other}, device_id_type=MESH)

    loads = [pltpu.make_async_copy(tokens_hbm, tok_v, load_sem.at[0])]
    for p, ref in enumerate((wg_hbm, wu_hbm, wd_hbm)):
        loads.append(pltpu.make_async_copy(ref, wf.at[p], load_sem.at[p + 1]))
    for copy in loads:
        copy.start()

    tok = tok_v.shape[0]
    lanes = 128
    experts = lax.broadcasted_iota(jnp.int32, (tok, lanes), 1).astype(F32)
    line = lax.broadcasted_iota(jnp.int32, (8, tok), 0)
    table = jnp.where(
        line == 0,
        routes_ref[0:1, :].astype(F32),
        jnp.where(
            line == 1,
            routes_ref[1:2, :].astype(F32),
            jnp.where(line == 2, logits_ref[0:1, :], logits_ref[1:2, :]),
        ),
    ).T
    first = table[:, 0:1]
    second = table[:, 1:2]
    is_first = first == experts
    is_second = second == experts
    marked = jnp.where(is_first | is_second, 1.0, 0.0).astype(BF16)
    earlier = jnp.where(
        lax.broadcasted_iota(jnp.int32, (tok, tok), 1)
        < lax.broadcasted_iota(jnp.int32, (tok, tok), 0),
        1.0,
        0.0,
    ).astype(BF16)
    before = jnp.dot(earlier, marked, preferred_element_type=F32)
    key_first = first * cap + jnp.sum(
        jnp.where(is_first, before, 0.0), axis=1, keepdims=True
    )
    key_second = second * cap + jnp.sum(
        jnp.where(is_second, before, 0.0), axis=1, keepdims=True
    )
    place = lax.broadcasted_iota(jnp.int32, (1, half * cap), 1)
    ident = place + cap * par
    for k in range(1, half):
        ident = ident + jnp.where(place >= k * cap, cap, 0)
    ident = ident.astype(F32)
    pick[0] = jnp.where(key_first == ident, 1.0, 0.0).astype(BF16)
    pick[1] = jnp.where(key_second == ident, 1.0, 0.0).astype(BF16)

    key_tab[0] = jnp.broadcast_to(key_first, (tok, lanes))
    key_tab[1] = jnp.broadcast_to(key_second, (tok, lanes))
    diff = table[:, 2:3] - table[:, 3:4]
    share_tab[0] = jnp.broadcast_to(1.0 / (1.0 + jnp.exp(-diff)), (tok, lanes))
    share_tab[1] = jnp.broadcast_to(1.0 / (1.0 + jnp.exp(diff)), (tok, lanes))

    loads[0].wait()
    chunk = 64

    def norm(i):
        at = pl.ds(pl.multiple_of(i * chunk, chunk), chunk)
        values = tok_v[at, :].astype(F32)
        mean = jnp.mean(values, axis=1, keepdims=True)
        centred = values - mean
        spread = jnp.mean(centred * centred, axis=1, keepdims=True)
        mine = tok_v[at, pl.ds(pl.multiple_of(y * feats, feats), feats)].astype(F32)
        normed_v[at, :] = ((mine - mean) * lax.rsqrt(spread + EPS)).astype(BF16)

    loop(0, tok // chunk, norm)
    picked = lax.dot_general(
        pick[0] + pick[1],
        normed_v[...],
        (((0,), (0,)), ((), ())),
        preferred_element_type=F32,
    )
    dsend[...] = picked.astype(BF16).reshape(dsend.shape)

    @pl.when(c == 0)
    def _():
        xb[y, lax.div(me, 2)] = dsend[lax.div(me, 2)]

    column = jnp.broadcast_to(gain_ref[...], (rows, rows)).T
    for copy in loads[1:]:
        copy.wait()

    def fold(e):
        wsend[e, 0] = (wf[0, e] * column).astype(BF16)
        wsend[e, 1] = (wf[1, e] * column).astype(BF16)
        wsend[e, 2] = wf[2, e].astype(BF16)

    loop(0, F, fold)
    for p in range(3):
        wown[p, me] = wsend[me, p]

    pl.semaphore_wait(barrier, F - 1 + G - 1 + 3)

    def tok_copy(k):
        return pltpu.make_async_remote_copy(
            src_ref=dsend.at[k],
            dst_ref=xb.at[y, lax.div(me, 2)],
            send_sem=tok_s,
            recv_sem=tok_r.at[lax.div(me, 2)],
            device_id={"fs": 2 * k + par},
            device_id_type=MESH,
        )

    def tok_arrival(k):
        return pltpu.make_async_remote_copy(
            src_ref=dsend.at[k],
            dst_ref=xb.at[y, k],
            send_sem=tok_s,
            recv_sem=tok_r.at[k],
            device_id={"fs": 2 * k + par},
            device_id_type=MESH,
        )

    kinds = (pl.ds(0, 2), pl.ds(2, 1))
    mine = pl.ds(pl.multiple_of(g * share, share), share)

    def z_copy(kind, to, source):
        return pltpu.make_async_remote_copy(
            src_ref=wsend.at[to, kinds[kind], mine],
            dst_ref=wown.at[kinds[kind], source, mine],
            send_sem=z_s,
            recv_sem=z_r.at[kind, source],
            device_id={"fs": to},
            device_id_type=MESH,
        )

    def x_copy(kind, s, n):
        at = wown.at[kinds[kind], s, mine]
        return pltpu.make_async_remote_copy(
            src_ref=at,
            dst_ref=at,
            send_sem=x_s.at[n - 1],
            recv_sem=x_r.at[kind, n - 1, s],
            device_id={"grp": lax.rem(g + n, G)},
            device_id_type=MESH,
        )

    def d_copy(kind, s):
        return pltpu.make_async_remote_copy(
            src_ref=wown.at[kinds[kind], s],
            dst_ref=wpart.at[kinds[kind], s],
            send_sem=d_s,
            recv_sem=d_r.at[kind * (s + 1)],
            device_id={"tp": partner},
            device_id_type=MESH,
        )

    def pass_on(kind, s):
        z_copy(kind, s, s).wait_recv()
        for n in range(1, G):
            x_copy(kind, s, n).start()

    def hand_over(kind, s):
        for n in range(1, G):
            x_copy(kind, s, n).wait_recv()
        d_copy(kind, s).start()

    def send_tok(k):
        @pl.when(lax.rem(k, 2) == par)
        def _():
            tok_copy(lax.div(k, 2)).start()

    def send_tok(m):
        k = lax.rem(lax.div(me, 2) + half // 2 + m, half)

        @pl.when(2 * k + par != me)
        def _():
            tok_copy(k).start()

    loop(0, half, send_tok)
    def send_weights(kind):
        loop(1, F, lambda m: z_copy(kind, lax.rem(me + offset(m), F), me).start())

    ahead = lax.rem(me + F - y, F)
    soon = (ahead >= F // 4 + 1) & (ahead <= F - F // 4)
    send_weights(0)

    @pl.when(soon)
    def _():
        send_weights(1)

    for kind in (0, 1):
        d_copy(kind, me).start()

    def source(m):
        return lax.rem(me + F - offset(m), F)

    def ag_copy(i, j, to_right):
        blk = lax.rem(y + Y - i, Y) if to_right else lax.rem(y + i, Y)
        at = xb.at[blk, pl.ds(j * per, per)]
        return pltpu.make_async_remote_copy(
            src_ref=at,
            dst_ref=at,
            send_sem=agr_s if to_right else agl_s,
            recv_sem=(agr_r if to_right else agl_r).at[i, j],
            device_id={"tp": right if to_right else left},
            device_id_type=MESH,
        )

    own_part = lax.div(lax.div(me, 2), per)
    near = [lax.rem(own_part + nsub + (j + 1) // 2 * (1 - j % 2 * 2), nsub) for j in range(nsub)]
    own_sum = lax.div(lax.div(me, 2), sum_per)
    far = [lax.rem(own_sum + nsum - 1 - j, nsum) for j in range(nsum)]

    for j in near:
        for n in range(per):
            k = j * per + n

            @pl.when(2 * k + par != me)
            def _(k=k):
                tok_arrival(k).wait_recv()

        ag_copy(0, j, True).start()
        ag_copy(0, j, False).start()

    def ag_step(i, both):
        for j in near:
            ag_copy(i - 1, j, True).wait_recv()
            ag_copy(i, j, True).start()
            ag_copy(i - 1, j, False).wait_recv()
            if both:
                ag_copy(i, j, False).start()

    def forward(act, kind, i):
        for m in (2 * i - 1, 2 * i):

            @pl.when((m > 0) & (m < F))
            def _(m=m):
                act(kind, source(m))

    def tend(i):
        forward(pass_on, 0, i)
        forward(hand_over, 0, i - 1)

    def middle(i):
        ag_step(i, True)
        tend(i)

    loop(1, left_steps, middle)
    for i in range(left_steps, right_steps):
        ag_step(i, i < left_steps)
        tend(i)

    @pl.when(jnp.logical_not(soon))
    def _():
        send_weights(1)

    loop(right_steps, F // 2 + 2, tend)
    def right_chunk(i):
        return lax.rem(y + right_steps + Y - i, Y)

    def left_chunk(i):
        return lax.rem(y + Y - left_steps + i, Y)

    def chunk_of(n):
        i = lax.div(n, 2)
        odd = lax.rem(n, 2)
        return lax.rem(y + Y + (1 - odd) * (right_steps - i) + odd * (i - left_steps), Y)

    def down_block(act, n):
        s = chunk_of(n)

        @pl.when((n < F) & (s != me))
        def _():
            act(1, s)

    def down_ready(i, both=True):
        for n in (2 * i + 4, 2 * i + 5):
            down_block(pass_on, n)
        for n in (2 * i + 2, 2 * i + 3):
            down_block(hand_over, n)
        d_copy(1, chunk_of(2 * i)).wait_recv()
        if both:
            d_copy(1, chunk_of(2 * i + 1)).wait_recv()

    for n in range(4):
        down_block(pass_on, n)
    taken(d_r.at[0], wpart.at[kinds[0]])
    store_g = pltpu.make_async_copy(wown.at[0], go_hbm.at[0], store_sem.at[0])
    store_u = pltpu.make_async_copy(wown.at[1], uo_hbm.at[0], store_sem.at[1])
    store_g.start()
    store_u.start()

    acc_g[...] = jnp.zeros_like(acc_g)
    acc_u[...] = jnp.zeros_like(acc_u)
    area = half * cap

    def contract(a, b):
        lhs = jnp.concatenate(
            [xb[a].reshape(area, feats), xb[b].reshape(area, feats)], axis=1
        )

        def rhs(p):
            top = jnp.concatenate([wown[p, a], wpart[p, a]], axis=1)
            low = jnp.concatenate([wown[p, b], wpart[p, b]], axis=1)
            return jnp.concatenate([top, low], axis=0)

        acc_g[...] += jnp.dot(lhs, rhs(0), preferred_element_type=F32)
        acc_u[...] += jnp.dot(lhs, rhs(1), preferred_element_type=F32)

    loop(1, left_steps + 1, lambda i: contract(lax.rem(y + Y - i, Y), lax.rem(y + i, Y)))
    for n in range(2):
        down_block(hand_over, n)
    for j in near:
        ag_copy(right_steps - 1, j, True).wait_recv()
    contract(y, lax.rem(y + right_steps, Y))

    def activate(k):
        at = pl.ds(pl.multiple_of(k * cap, cap), cap)
        v = acc_g[at, :]
        hid[at, :] = (v / (1.0 + jnp.exp(-v)) * acc_u[at, :]).astype(BF16)

    loop(0, half, activate)

    def product(d):
        block = jnp.concatenate([wown[2, d], wpart[2, d]], axis=1)
        return lax.dot_general(
            hid[...], block, (((1,), (1,)), ((), ())), preferred_element_type=F32
        )

    sub = sum_per * cap
    down_ready(0)

    def near_copy(n):
        return pltpu.make_async_remote_copy(
            src_ref=near_send.at[n],
            dst_ref=near_recv.at[n],
            send_sem=near_s,
            recv_sem=near_r.at[n],
            device_id={"tp": partner},
            device_id_type=MESH,
        )

    def rs_copy(i, h, j, to_right):
        return pltpu.make_async_remote_copy(
            src_ref=(rs_rsend if to_right else rs_lsend).at[i, h, j],
            dst_ref=(rs_rrecv if to_right else rs_lrecv).at[i, h, j],
            send_sem=rsr_s if to_right else rsl_s,
            recv_sem=(rsr_r if to_right else rsl_r).at[i, h, j],
            device_id={"tp": right if to_right else left},
            device_id_type=MESH,
        )

    def ret_copy(h, k):
        return pltpu.make_async_remote_copy(
            src_ref=ret_send.at[h, k],
            dst_ref=ret_recv.at[me],
            send_sem=ret_s,
            recv_sem=ret_r,
            device_id={"fs": 2 * k + lax.rem(me + h, 2)},
            device_id_type=MESH,
        )

    swap = pltpu.make_async_remote_copy(
        src_ref=mix_own,
        dst_ref=mix_other,
        send_sem=mix_s,
        recv_sem=mix_r,
        device_id={"tp": partner},
        device_id_type=MESH,
    )

    @pl.when(c == 0)
    def _():
        def give(n):
            near_send[n] = product(chunk_of(n)).astype(BF16)
            near_copy(n).start()

        give(0)
        give(1)

        def give_two(i):
            down_ready(i)
            give(2 * i)
            give(2 * i + 1)

        loop(1, right_steps, give_two)

    @pl.when(c == 1)
    def _():
        def rows_of(j):
            return pl.ds(pl.multiple_of(j * sub, sub), sub)

        def terms(i, both):
            part_r[...] = product(right_chunk(i))
            if both:
                part_l[...] = product(left_chunk(i))

        def others(i):
            near_copy(2 * i).wait_recv()
            near_copy(2 * i + 1).wait_recv()

        def term(h, n, part, j):
            return part[rows_of(j), :] if h else near_recv[n, rows_of(j), :].astype(F32)

        terms(0, True)
        for h in (1, 0):
            if h == 0:
                others(0)
            for j in far:
                rs_rsend[0, h, j] = term(h, 0, part_r, j).astype(BF16)
                rs_copy(0, h, j, True).start()
                rs_lsend[0, h, j] = term(h, 1, part_l, j).astype(BF16)
                rs_copy(0, h, j, False).start()

        def rs_step(i, both):
            down_ready(i)
            terms(i, both)
            for h in (1, 0):
                if h == 0:
                    others(i)
                for j in far:
                    rs_copy(i - 1, h, j, True).wait_recv()
                    rs_rsend[i, h, j] = (
                        rs_rrecv[i - 1, h, j].astype(F32) + term(h, 2 * i, part_r, j)
                    ).astype(BF16)
                    rs_copy(i, h, j, True).start()
                    if both:
                        rs_copy(i - 1, h, j, False).wait_recv()
                        rs_lsend[i, h, j] = (
                            rs_lrecv[i - 1, h, j].astype(F32) + term(h, 2 * i + 1, part_l, j)
                        ).astype(BF16)
                        rs_copy(i, h, j, False).start()

        loop(1, left_steps, lambda i: rs_step(i, True))
        for i in range(max(1, left_steps), right_steps):
            rs_step(i, False)

        part_r[...] = product(y)
        for h in (1, 0):
            for j in far:
                rs_copy(left_steps - 1, h, j, False).wait_recv()
                rs_copy(right_steps - 1, h, j, True).wait_recv()
                total = (
                    term(h, F - 1, part_r, j)
                    + rs_rrecv[right_steps - 1, h, j].astype(F32)
                    + rs_lrecv[left_steps - 1, h, j].astype(F32)
                ).astype(BF16)
                ret_send[h, pl.ds(j * sum_per, sum_per)] = total.reshape(sum_per, cap, feats)
                for n in range(sum_per):
                    k = j * sum_per + n

                    @pl.when(2 * k + lax.rem(me + h, 2) != me)
                    def _(h=h, k=k):
                        ret_copy(h, k).start()

        ret_recv[me] = ret_send[0, lax.div(me, 2)]
        slots = lax.broadcasted_iota(jnp.int32, (1, F * cap), 1).astype(F32)
        chosen = [jnp.where(key_tab[n, :, 0:1] == slots, 1.0, 0.0).astype(BF16) for n in (0, 1)]
        taken(ret_r, ret_recv.at[pl.ds(0, F - 1)])
        returned = ret_recv[...].reshape(F * cap, feats)
        both = (
            share_tab[0] * jnp.dot(chosen[0], returned, preferred_element_type=F32)
            + share_tab[1] * jnp.dot(chosen[1], returned, preferred_element_type=F32)
        ).T.astype(BF16)
        width = mix_ref.shape[0]
        mix_own[...] = both[:width, :]
        swap.start()
        mix_ref[...] = both[width:, :]

    store_d = pltpu.make_async_copy(wown.at[2], do_hbm.at[0], store_sem.at[2])
    store_d.start()

    @pl.when(c == 0)
    def _():
        swap.wait_recv()
        mix_ref[...] = mix_other[...]

    for copy in (store_g, store_u, store_d):
        copy.wait()
    taken(z_s, wsend.at[pl.ds(0, F - 1), :, mine])
    for n in range(1, G):
        taken(x_s.at[n - 1], wown.at[:, pl.ds(0, F - 1), mine])
    taken(d_s, wown)
    taken(agr_s, xb.at[pl.ds(0, right_steps)])
    taken(agl_s, xb.at[pl.ds(0, left_steps)])

    @pl.when(c == 0)
    def _():
        taken(tok_s, dsend.at[pl.ds(0, half - 1)])
        taken(near_s, near_send)

    @pl.when(c == 1)
    def _():
        taken(tok_s, dsend)
        swap.wait_send()
        taken(ret_s, ret_recv.at[pl.ds(0, F - 1)])
        taken(rsr_s, rs_rsend)
        taken(rsl_s, rs_lsend)


def hand_in(n, *refs):
    sources, results, holds, sems = refs[:n], refs[n : 2 * n], refs[2 * n : 3 * n], refs[3 * n]
    ins = [pltpu.make_async_copy(sources[i], holds[i], sems.at[0, i]) for i in range(n)]
    outs = [pltpu.make_async_copy(holds[i], results[i], sems.at[1, i]) for i in range(n)]
    for copy in ins:
        copy.start()
    for i in range(n):
        ins[i].wait()
        outs[i].start()
    for copy in outs:
        copy.wait()


def solution(mesh):
    G, F, Y = mesh.shape["grp"], mesh.shape["fs"], mesh.shape["tp"] // 2

    def on_device(tokens, routes, route_logits, gain, w_gate, w_up, w_down):
        experts, rows, cols = w_gate.shape
        tok, width = tokens.shape
        cap = 3 * tok // experts
        half = F // 2
        nsub, nsum = min(4, half), min(2, half)
        feats = width // Y
        area = half * cap
        rs, ls = Y // 2, Y // 2 - 1
        any_spec = pl.BlockSpec(memory_space=pl.ANY)
        vmem = pl.BlockSpec(memory_space=pltpu.VMEM)
        dma = pltpu.SemaphoreType.DMA
        out = jax.ShapeDtypeStruct((1, F, rows, cols), BF16)
        made = pl.pallas_call(
            functools.partial(kernel, (G, F, Y, cap, nsub, nsum)),
            out_shape=(out, out, out, jax.ShapeDtypeStruct((feats // 2, tok), BF16)),
            in_specs=[any_spec, vmem, vmem, vmem, any_spec, any_spec, any_spec],
            out_specs=(any_spec, any_spec, any_spec, vmem),
            scratch_shapes=[
                pltpu.VMEM((tok, width), BF16),
                pltpu.VMEM((tok, feats), BF16),
                pltpu.VMEM((3, F, rows, cols), F32),
                pltpu.VMEM((F, 3, rows, cols), BF16),
                pltpu.VMEM((3, F, rows, cols), BF16),
                pltpu.VMEM((3, F, rows, cols), BF16),
                pltpu.VMEM((Y, half, cap, feats), BF16),
                pltpu.VMEM((half, cap, feats), BF16),
                pltpu.VMEM((2, tok, area), BF16),
                pltpu.VMEM((area, 2 * cols), BF16),
                pltpu.VMEM((area, 2 * cols), F32),
                pltpu.VMEM((area, 2 * cols), F32),
                pltpu.VMEM((area, feats), F32),
                pltpu.VMEM((area, feats), F32),
                pltpu.VMEM((rs, 2, nsum, area // nsum, feats), BF16),
                pltpu.VMEM((ls, 2, nsum, area // nsum, feats), BF16),
                pltpu.VMEM((rs, 2, nsum, area // nsum, feats), BF16),
                pltpu.VMEM((ls, 2, nsum, area // nsum, feats), BF16),
                pltpu.VMEM((F, area, feats), BF16),
                pltpu.VMEM((F, area, feats), BF16),
                pltpu.VMEM((2, half, cap, feats), BF16),
                pltpu.VMEM((F, cap, feats), BF16),
                pltpu.VMEM((2, tok, feats), F32),
                pltpu.VMEM((2, tok, feats), F32),
                pltpu.VMEM((feats // 2, tok), BF16),
                pltpu.VMEM((feats // 2, tok), BF16),
                dma((4,)),
                dma((3,)),
                dma,
                dma((half,)),
                dma,
                dma((2, F)),
                dma((max(G - 1, 1),)),
                dma((2, max(G - 1, 1), F)),
                dma,
                dma((F + 1,)),
                dma,
                dma((rs, nsub)),
                dma,
                dma((ls, nsub)),
                dma,
                dma((F,)),
                dma,
                dma((rs, 2, nsum)),
                dma,
                dma((ls, 2, nsum)),
                dma,
                dma,
                dma,
                dma,
            ],
            compiler_params=pltpu.CompilerParams(collective_id=0, has_side_effects=True),
        )(tokens, routes.T, route_logits.T, gain.reshape(1, rows), w_gate, w_up, w_down)
        gate_out, up_out, down_out, mixed = pl.pallas_call(
            functools.partial(hand_in, 4),
            out_shape=[jax.ShapeDtypeStruct(a.shape, a.dtype) for a in made],
            in_specs=[any_spec] * 4,
            out_specs=[any_spec] * 4,
            scratch_shapes=[pltpu.VMEM(a.shape, a.dtype) for a in made] + [dma((2, 4))],
        )(*made)
        weights = tuple(w.reshape(1, F * rows, cols) for w in (gate_out, up_out, down_out))
        return (*weights, mixed.T)

    in_specs = (
        P(("grp", "fs"), None),
        P(("grp", "fs"), None),
        P(("grp", "fs"), None),
        P("fs"),
        P(None, "fs", "tp"),
        P(None, "fs", "tp"),
        P(None, "fs", "tp"),
    )
    out_specs = (
        P(("grp", "fs"), None, "tp"),
        P(("grp", "fs"), None, "tp"),
        P(("grp", "fs"), None, "tp"),
        P(("grp", "fs"), "tp"),
    )
    return jax.shard_map(
        on_device, mesh=mesh, in_specs=in_specs, out_specs=out_specs, check_vma=False
    )
```

```python
import functools

import jax
import jax.numpy as jnp
from jax import lax
from jax.experimental import pallas as pl
from jax.experimental.pallas import tpu as pltpu
from jax.sharding import PartitionSpec as P

EPS = 1e-06
MESH = pl.DeviceIdType.MESH
F32 = jnp.float32
BF16 = jnp.bfloat16


def loop(lo, hi, body):
    def step(i, carry):
        body(i)
        return carry

    lax.fori_loop(lo, hi, step, 0)


def kernel(
    dims,
    tokens_hbm,
    routes_ref,
    logits_ref,
    gain_ref,
    wg_hbm,
    wu_hbm,
    wd_hbm,
    go_hbm,
    uo_hbm,
    do_hbm,
    mix_ref,
    tok_v,
    normed_v,
    wf,
    wsend,
    wown,
    wpart,
    xb,
    dsend,
    pick,
    hid,
    acc_g,
    acc_u,
    part_r,
    part_l,
    rs_rsend,
    rs_lsend,
    rs_rrecv,
    rs_lrecv,
    near_send,
    near_recv,
    ret_send,
    ret_recv,
    key_tab,
    share_tab,
    mix_own,
    mix_other,
    load_sem,
    store_sem,
    tok_s,
    tok_r,
    z_s,
    z_r,
    x_s,
    x_r,
    d_s,
    d_r,
    agr_s,
    agr_r,
    agl_s,
    agl_r,
    near_s,
    near_r,
    rsr_s,
    rsr_r,
    rsl_s,
    rsl_r,
    ret_s,
    ret_r,
    mix_s,
    mix_r,
):
    G, F, Y, cap, nsub, nsum = dims
    half = F // 2
    per = half // nsub
    sum_per = half // nsum
    right_steps, left_steps = Y // 2, Y // 2 - 1
    rows = wsend.shape[2]
    share = rows // G
    feats = xb.shape[3]

    g = lax.axis_index("grp")
    me = lax.axis_index("fs")
    t = lax.axis_index("tp")
    y = lax.div(t, 2)
    c = lax.rem(t, 2)
    partner = t + 1 - 2 * c
    right = lax.rem(y + 1, Y) * 2 + c
    left = lax.rem(y + Y - 1, Y) * 2 + c
    par = lax.rem(me + c, 2)

    def taken(sem, refs):
        pltpu.make_async_copy(refs, refs, sem).wait()

    def offset(m):
        step = lax.div(m + 1, 2)
        odd = lax.rem(m, 2)
        return odd * step + (1 - odd) * (F - step)

    barrier = pltpu.get_barrier_semaphore()

    def greet(m):
        pl.semaphore_signal(
            barrier, inc=1, device_id={"fs": lax.rem(me + m, F)}, device_id_type=MESH
        )

    loop(1, F, greet)
    for m in range(1, G):
        pl.semaphore_signal(
            barrier, inc=1, device_id={"grp": lax.rem(g + m, G)}, device_id_type=MESH
        )
    for other in (partner, left, right):
        pl.semaphore_signal(barrier, inc=1, device_id={"tp": other}, device_id_type=MESH)

    loads = [pltpu.make_async_copy(tokens_hbm, tok_v, load_sem.at[0])]
    for p, ref in enumerate((wg_hbm, wu_hbm, wd_hbm)):
        loads.append(pltpu.make_async_copy(ref, wf.at[p], load_sem.at[p + 1]))
    for copy in loads:
        copy.start()

    tok = tok_v.shape[0]
    lanes = 128
    experts = lax.broadcasted_iota(jnp.int32, (tok, lanes), 1).astype(F32)
    line = lax.broadcasted_iota(jnp.int32, (8, tok), 0)
    table = jnp.where(
        line == 0,
        routes_ref[0:1, :].astype(F32),
        jnp.where(
            line == 1,
            routes_ref[1:2, :].astype(F32),
            jnp.where(line == 2, logits_ref[0:1, :], logits_ref[1:2, :]),
        ),
    ).T
    first = table[:, 0:1]
    second = table[:, 1:2]
    is_first = first == experts
    is_second = second == experts
    marked = jnp.where(is_first | is_second, 1.0, 0.0).astype(BF16)
    earlier = jnp.where(
        lax.broadcasted_iota(jnp.int32, (tok, tok), 1)
        < lax.broadcasted_iota(jnp.int32, (tok, tok), 0),
        1.0,
        0.0,
    ).astype(BF16)
    before = jnp.dot(earlier, marked, preferred_element_type=F32)
    key_first = first * cap + jnp.sum(
        jnp.where(is_first, before, 0.0), axis=1, keepdims=True
    )
    key_second = second * cap + jnp.sum(
        jnp.where(is_second, before, 0.0), axis=1, keepdims=True
    )
    place = lax.broadcasted_iota(jnp.int32, (1, half * cap), 1)
    ident = place + cap * par
    for k in range(1, half):
        ident = ident + jnp.where(place >= k * cap, cap, 0)
    ident = ident.astype(F32)
    pick[0] = jnp.where(key_first == ident, 1.0, 0.0).astype(BF16)
    pick[1] = jnp.where(key_second == ident, 1.0, 0.0).astype(BF16)

    key_tab[0] = jnp.broadcast_to(key_first, (tok, lanes))
    key_tab[1] = jnp.broadcast_to(key_second, (tok, lanes))
    diff = table[:, 2:3] - table[:, 3:4]
    share_tab[0] = jnp.broadcast_to(1.0 / (1.0 + jnp.exp(-diff)), (tok, lanes))
    share_tab[1] = jnp.broadcast_to(1.0 / (1.0 + jnp.exp(diff)), (tok, lanes))

    loads[0].wait()
    chunk = 64

    def norm(i):
        at = pl.ds(pl.multiple_of(i * chunk, chunk), chunk)
        values = tok_v[at, :].astype(F32)
        mean = jnp.mean(values, axis=1, keepdims=True)
        centred = values - mean
        spread = jnp.mean(centred * centred, axis=1, keepdims=True)
        mine = tok_v[at, pl.ds(pl.multiple_of(y * feats, feats), feats)].astype(F32)
        normed_v[at, :] = ((mine - mean) * lax.rsqrt(spread + EPS)).astype(BF16)

    loop(0, tok // chunk, norm)
    picked = lax.dot_general(
        pick[0] + pick[1],
        normed_v[...],
        (((0,), (0,)), ((), ())),
        preferred_element_type=F32,
    )
    dsend[...] = picked.astype(BF16).reshape(dsend.shape)

    @pl.when(c == 0)
    def _():
        xb[y, lax.div(me, 2)] = dsend[lax.div(me, 2)]

    column = jnp.broadcast_to(gain_ref[...], (rows, rows)).T
    for copy in loads[1:]:
        copy.wait()

    def fold(e):
        wsend[e, 0] = (wf[0, e] * column).astype(BF16)
        wsend[e, 1] = (wf[1, e] * column).astype(BF16)
        wsend[e, 2] = wf[2, e].astype(BF16)

    loop(0, F, fold)
    for p in range(3):
        wown[p, me] = wsend[me, p]

    pl.semaphore_wait(barrier, F - 1 + G - 1 + 3)

    def tok_copy(k):
        return pltpu.make_async_remote_copy(
            src_ref=dsend.at[k],
            dst_ref=xb.at[y, lax.div(me, 2)],
            send_sem=tok_s,
            recv_sem=tok_r.at[lax.div(me, 2)],
            device_id={"fs": 2 * k + par},
            device_id_type=MESH,
        )

    def tok_arrival(k):
        return pltpu.make_async_remote_copy(
            src_ref=dsend.at[k],
            dst_ref=xb.at[y, k],
            send_sem=tok_s,
            recv_sem=tok_r.at[k],
            device_id={"fs": 2 * k + par},
            device_id_type=MESH,
        )

    kinds = (pl.ds(0, 2), pl.ds(2, 1))
    mine = pl.ds(pl.multiple_of(g * share, share), share)

    def z_copy(kind, to, source):
        return pltpu.make_async_remote_copy(
            src_ref=wsend.at[to, kinds[kind], mine],
            dst_ref=wown.at[kinds[kind], source, mine],
            send_sem=z_s,
            recv_sem=z_r.at[kind, source],
            device_id={"fs": to},
            device_id_type=MESH,
        )

    def x_copy(kind, s, n):
        at = wown.at[kinds[kind], s, mine]
        return pltpu.make_async_remote_copy(
            src_ref=at,
            dst_ref=at,
            send_sem=x_s.at[n - 1],
            recv_sem=x_r.at[kind, n - 1, s],
            device_id={"grp": lax.rem(g + n, G)},
            device_id_type=MESH,
        )

    def d_copy(kind, s):
        return pltpu.make_async_remote_copy(
            src_ref=wown.at[kinds[kind], s],
            dst_ref=wpart.at[kinds[kind], s],
            send_sem=d_s,
            recv_sem=d_r.at[kind, s],
            device_id={"tp": partner},
            device_id_type=MESH,
        )

    def pass_on(kind, s):
        z_copy(kind, s, s).wait_recv()
        for n in range(1, G):
            x_copy(kind, s, n).start()

    def hand_over(kind, s):
        for n in range(1, G):
            x_copy(kind, s, n).wait_recv()
        d_copy(kind, s).start()

    def send_tok(k):
        @pl.when(lax.rem(k, 2) == par)
        def _():
            tok_copy(lax.div(k, 2)).start()

    def send_tok(m):
        k = lax.rem(lax.div(me, 2) + half // 2 + m, half)

        @pl.when(2 * k + par != me)
        def _():
            tok_copy(k).start()

    loop(0, half, send_tok)
    def send_weights(kind):
        loop(1, F, lambda m: z_copy(kind, lax.rem(me + offset(m), F), me).start())

    ahead = lax.rem(me + F - y, F)
    soon = (ahead >= F // 4 + 1) & (ahead <= F - F // 4)
    send_weights(0)

    @pl.when(soon)
    def _():
        send_weights(1)

    for kind in (0, 1):
        d_copy(kind, me).start()

    def source(m):
        return lax.rem(me + F - offset(m), F)

    def ag_copy(i, j, to_right):
        blk = lax.rem(y + Y - i, Y) if to_right else lax.rem(y + i, Y)
        at = xb.at[blk, pl.ds(j * per, per)]
        return pltpu.make_async_remote_copy(
            src_ref=at,
            dst_ref=at,
            send_sem=agr_s if to_right else agl_s,
            recv_sem=(agr_r if to_right else agl_r).at[i, j],
            device_id={"tp": right if to_right else left},
            device_id_type=MESH,
        )

    own_part = lax.div(lax.div(me, 2), per)
    near = [lax.rem(own_part + nsub + (j + 1) // 2 * (1 - j % 2 * 2), nsub) for j in range(nsub)]
    own_sum = lax.div(lax.div(me, 2), sum_per)
    far = [lax.rem(own_sum + nsum - 1 - j, nsum) for j in range(nsum)]

    for j in near:
        for n in range(per):
            k = j * per + n

            @pl.when(2 * k + par != me)
            def _(k=k):
                tok_arrival(k).wait_recv()

        ag_copy(0, j, True).start()
        ag_copy(0, j, False).start()

    def ag_step(i, both):
        for j in near:
            ag_copy(i - 1, j, True).wait_recv()
            ag_copy(i, j, True).start()
            ag_copy(i - 1, j, False).wait_recv()
            if both:
                ag_copy(i, j, False).start()

    def forward(act, kind, i):
        for m in (2 * i - 1, 2 * i):

            @pl.when((m > 0) & (m < F))
            def _(m=m):
                act(kind, source(m))

    def tend(i):
        forward(pass_on, 0, i)
        forward(hand_over, 0, i - 1)

    def middle(i):
        ag_step(i, True)
        tend(i)

    loop(1, left_steps, middle)
    for i in range(left_steps, right_steps):
        ag_step(i, i < left_steps)
        tend(i)

    @pl.when(jnp.logical_not(soon))
    def _():
        send_weights(1)

    tend(right_steps)

    acc_g[...] = jnp.zeros_like(acc_g)
    acc_u[...] = jnp.zeros_like(acc_u)
    area = half * cap

    def contract(a, b):
        lhs = jnp.concatenate(
            [xb[a].reshape(area, feats), xb[b].reshape(area, feats)], axis=1
        )

        def rhs(p):
            top = jnp.concatenate([wown[p, a], wpart[p, a]], axis=1)
            low = jnp.concatenate([wown[p, b], wpart[p, b]], axis=1)
            return jnp.concatenate([top, low], axis=0)

        acc_g[...] += jnp.dot(lhs, rhs(0), preferred_element_type=F32)
        acc_u[...] += jnp.dot(lhs, rhs(1), preferred_element_type=F32)

    def contract_pair(i):
        a, b = lax.rem(me + i, F), lax.rem(me + F - i, F)
        d_copy(0, a).wait_recv()
        d_copy(0, b).wait_recv()
        contract(a, b)

    for j in near:
        ag_copy(right_steps - 1, j, True).wait_recv()
    pairs = max(1, left_steps - 1)
    loop(1, pairs, contract_pair)
    loop(right_steps + 1, F // 2 + 2, tend)

    def right_chunk(i):
        return lax.rem(y + right_steps + Y - i, Y)

    def left_chunk(i):
        return lax.rem(y + Y - left_steps + i, Y)

    def chunk_of(n):
        i = lax.div(n, 2)
        odd = lax.rem(n, 2)
        return lax.rem(y + Y + (1 - odd) * (right_steps - i) + odd * (i - left_steps), Y)

    def down_block(act, n):
        s = chunk_of(n)

        @pl.when((n < F) & (s != me))
        def _():
            act(1, s)

    def down_ready(i, both=True):
        for n in (2 * i + 4, 2 * i + 5):
            down_block(pass_on, n)
        for n in (2 * i + 2, 2 * i + 3):
            down_block(hand_over, n)
        d_copy(1, chunk_of(2 * i)).wait_recv()
        if both:
            d_copy(1, chunk_of(2 * i + 1)).wait_recv()

    for n in range(4):
        down_block(pass_on, n)
    store_g = pltpu.make_async_copy(wown.at[0], go_hbm.at[0], store_sem.at[0])
    store_u = pltpu.make_async_copy(wown.at[1], uo_hbm.at[0], store_sem.at[1])
    store_g.start()
    store_u.start()

    loop(pairs, left_steps + 1, contract_pair)
    for n in range(2):
        down_block(hand_over, n)
    opposite = lax.rem(me + right_steps, F)
    d_copy(0, me).wait_recv()
    d_copy(0, opposite).wait_recv()
    contract(me, opposite)

    def activate(k):
        at = pl.ds(pl.multiple_of(k * cap, cap), cap)
        v = acc_g[at, :]
        hid[at, :] = (v / (1.0 + jnp.exp(-v)) * acc_u[at, :]).astype(BF16)

    loop(0, half, activate)

    def product(d):
        block = jnp.concatenate([wown[2, d], wpart[2, d]], axis=1)
        return lax.dot_general(
            hid[...], block, (((1,), (1,)), ((), ())), preferred_element_type=F32
        )

    sub = sum_per * cap
    down_ready(0)

    def near_copy(n):
        return pltpu.make_async_remote_copy(
            src_ref=near_send.at[n],
            dst_ref=near_recv.at[n],
            send_sem=near_s,
            recv_sem=near_r.at[n],
            device_id={"tp": partner},
            device_id_type=MESH,
        )

    def rs_copy(i, h, j, to_right):
        return pltpu.make_async_remote_copy(
            src_ref=(rs_rsend if to_right else rs_lsend).at[i, h, j],
            dst_ref=(rs_rrecv if to_right else rs_lrecv).at[i, h, j],
            send_sem=rsr_s if to_right else rsl_s,
            recv_sem=(rsr_r if to_right else rsl_r).at[i, h, j],
            device_id={"tp": right if to_right else left},
            device_id_type=MESH,
        )

    def ret_copy(h, k):
        return pltpu.make_async_remote_copy(
            src_ref=ret_send.at[h, k],
            dst_ref=ret_recv.at[me],
            send_sem=ret_s,
            recv_sem=ret_r,
            device_id={"fs": 2 * k + lax.rem(me + h, 2)},
            device_id_type=MESH,
        )

    swap = pltpu.make_async_remote_copy(
        src_ref=mix_own,
        dst_ref=mix_other,
        send_sem=mix_s,
        recv_sem=mix_r,
        device_id={"tp": partner},
        device_id_type=MESH,
    )

    @pl.when(c == 0)
    def _():
        def give(n):
            near_send[n] = product(chunk_of(n)).astype(BF16)
            near_copy(n).start()

        give(0)
        give(1)

        def give_two(i):
            down_ready(i)
            give(2 * i)
            give(2 * i + 1)

        loop(1, right_steps, give_two)

    @pl.when(c == 1)
    def _():
        def rows_of(j):
            return pl.ds(pl.multiple_of(j * sub, sub), sub)

        def terms(i, both):
            part_r[...] = product(right_chunk(i))
            if both:
                part_l[...] = product(left_chunk(i))

        def others(i):
            near_copy(2 * i).wait_recv()
            near_copy(2 * i + 1).wait_recv()

        def term(h, n, part, j):
            return part[rows_of(j), :] if h else near_recv[n, rows_of(j), :].astype(F32)

        terms(0, True)
        for h in (1, 0):
            if h == 0:
                others(0)
            for j in far:
                rs_rsend[0, h, j] = term(h, 0, part_r, j).astype(BF16)
                rs_copy(0, h, j, True).start()
                rs_lsend[0, h, j] = term(h, 1, part_l, j).astype(BF16)
                rs_copy(0, h, j, False).start()

        def rs_step(i, both):
            down_ready(i)
            terms(i, both)
            for h in (1, 0):
                if h == 0:
                    others(i)
                for j in far:
                    rs_copy(i - 1, h, j, True).wait_recv()
                    rs_rsend[i, h, j] = (
                        rs_rrecv[i - 1, h, j].astype(F32) + term(h, 2 * i, part_r, j)
                    ).astype(BF16)
                    rs_copy(i, h, j, True).start()
                    if both:
                        rs_copy(i - 1, h, j, False).wait_recv()
                        rs_lsend[i, h, j] = (
                            rs_lrecv[i - 1, h, j].astype(F32) + term(h, 2 * i + 1, part_l, j)
                        ).astype(BF16)
                        rs_copy(i, h, j, False).start()

        loop(1, left_steps, lambda i: rs_step(i, True))
        for i in range(max(1, left_steps), right_steps):
            rs_step(i, False)

        part_r[...] = product(y)
        for h in (1, 0):
            for j in far:
                rs_copy(left_steps - 1, h, j, False).wait_recv()
                rs_copy(right_steps - 1, h, j, True).wait_recv()
                total = (
                    term(h, F - 1, part_r, j)
                    + rs_rrecv[right_steps - 1, h, j].astype(F32)
                    + rs_lrecv[left_steps - 1, h, j].astype(F32)
                ).astype(BF16)
                ret_send[h, pl.ds(j * sum_per, sum_per)] = total.reshape(sum_per, cap, feats)
                for n in range(sum_per):
                    k = j * sum_per + n

                    @pl.when(2 * k + lax.rem(me + h, 2) != me)
                    def _(h=h, k=k):
                        ret_copy(h, k).start()

        ret_recv[me] = ret_send[0, lax.div(me, 2)]
        slots = lax.broadcasted_iota(jnp.int32, (1, F * cap), 1).astype(F32)
        chosen = [jnp.where(key_tab[n, :, 0:1] == slots, 1.0, 0.0).astype(BF16) for n in (0, 1)]
        taken(ret_r, ret_recv.at[pl.ds(0, F - 1)])
        returned = ret_recv[...].reshape(F * cap, feats)
        both = (
            share_tab[0] * jnp.dot(chosen[0], returned, preferred_element_type=F32)
            + share_tab[1] * jnp.dot(chosen[1], returned, preferred_element_type=F32)
        ).T.astype(BF16)
        width = mix_ref.shape[0]
        mix_own[...] = both[:width, :]
        swap.start()
        mix_ref[...] = both[width:, :]

    store_d = pltpu.make_async_copy(wown.at[2], do_hbm.at[0], store_sem.at[2])
    store_d.start()

    @pl.when(c == 0)
    def _():
        swap.wait_recv()
        mix_ref[...] = mix_other[...]

    for copy in (store_g, store_u, store_d):
        copy.wait()
    taken(z_s, wsend.at[pl.ds(0, F - 1), :, mine])
    for n in range(1, G):
        taken(x_s.at[n - 1], wown.at[:, pl.ds(0, F - 1), mine])
    taken(d_s, wown)
    taken(agr_s, xb.at[pl.ds(0, right_steps)])
    taken(agl_s, xb.at[pl.ds(0, left_steps)])

    @pl.when(c == 0)
    def _():
        taken(tok_s, dsend.at[pl.ds(0, half - 1)])
        taken(near_s, near_send)

    @pl.when(c == 1)
    def _():
        taken(tok_s, dsend)
        swap.wait_send()
        taken(ret_s, ret_recv.at[pl.ds(0, F - 1)])
        taken(rsr_s, rs_rsend)
        taken(rsl_s, rs_lsend)


def hand_in(n, *refs):
    sources, results, holds, sems = refs[:n], refs[n : 2 * n], refs[2 * n : 3 * n], refs[3 * n]
    ins = [pltpu.make_async_copy(sources[i], holds[i], sems.at[0, i]) for i in range(n)]
    outs = [pltpu.make_async_copy(holds[i], results[i], sems.at[1, i]) for i in range(n)]
    for copy in ins:
        copy.start()
    for i in range(n):
        ins[i].wait()
        outs[i].start()
    for copy in outs:
        copy.wait()


def solution(mesh):
    G, F, Y = mesh.shape["grp"], mesh.shape["fs"], mesh.shape["tp"] // 2

    def on_device(tokens, routes, route_logits, gain, w_gate, w_up, w_down):
        experts, rows, cols = w_gate.shape
        tok, width = tokens.shape
        cap = 3 * tok // experts
        half = F // 2
        nsub, nsum = min(4, half), min(2, half)
        feats = width // Y
        area = half * cap
        rs, ls = Y // 2, Y // 2 - 1
        any_spec = pl.BlockSpec(memory_space=pl.ANY)
        vmem = pl.BlockSpec(memory_space=pltpu.VMEM)
        dma = pltpu.SemaphoreType.DMA
        out = jax.ShapeDtypeStruct((1, F, rows, cols), BF16)
        made = pl.pallas_call(
            functools.partial(kernel, (G, F, Y, cap, nsub, nsum)),
            out_shape=(out, out, out, jax.ShapeDtypeStruct((feats // 2, tok), BF16)),
            in_specs=[any_spec, vmem, vmem, vmem, any_spec, any_spec, any_spec],
            out_specs=(any_spec, any_spec, any_spec, vmem),
            scratch_shapes=[
                pltpu.VMEM((tok, width), BF16),
                pltpu.VMEM((tok, feats), BF16),
                pltpu.VMEM((3, F, rows, cols), F32),
                pltpu.VMEM((F, 3, rows, cols), BF16),
                pltpu.VMEM((3, F, rows, cols), BF16),
                pltpu.VMEM((3, F, rows, cols), BF16),
                pltpu.VMEM((Y, half, cap, feats), BF16),
                pltpu.VMEM((half, cap, feats), BF16),
                pltpu.VMEM((2, tok, area), BF16),
                pltpu.VMEM((area, 2 * cols), BF16),
                pltpu.VMEM((area, 2 * cols), F32),
                pltpu.VMEM((area, 2 * cols), F32),
                pltpu.VMEM((area, feats), F32),
                pltpu.VMEM((area, feats), F32),
                pltpu.VMEM((rs, 2, nsum, area // nsum, feats), BF16),
                pltpu.VMEM((ls, 2, nsum, area // nsum, feats), BF16),
                pltpu.VMEM((rs, 2, nsum, area // nsum, feats), BF16),
                pltpu.VMEM((ls, 2, nsum, area // nsum, feats), BF16),
                pltpu.VMEM((F, area, feats), BF16),
                pltpu.VMEM((F, area, feats), BF16),
                pltpu.VMEM((2, half, cap, feats), BF16),
                pltpu.VMEM((F, cap, feats), BF16),
                pltpu.VMEM((2, tok, feats), F32),
                pltpu.VMEM((2, tok, feats), F32),
                pltpu.VMEM((feats // 2, tok), BF16),
                pltpu.VMEM((feats // 2, tok), BF16),
                dma((4,)),
                dma((3,)),
                dma,
                dma((half,)),
                dma,
                dma((2, F)),
                dma((max(G - 1, 1),)),
                dma((2, max(G - 1, 1), F)),
                dma,
                dma((2, F)),
                dma,
                dma((rs, nsub)),
                dma,
                dma((ls, nsub)),
                dma,
                dma((F,)),
                dma,
                dma((rs, 2, nsum)),
                dma,
                dma((ls, 2, nsum)),
                dma,
                dma,
                dma,
                dma,
            ],
            compiler_params=pltpu.CompilerParams(collective_id=0, has_side_effects=True),
        )(tokens, routes.T, route_logits.T, gain.reshape(1, rows), w_gate, w_up, w_down)
        gate_out, up_out, down_out, mixed = pl.pallas_call(
            functools.partial(hand_in, 4),
            out_shape=[jax.ShapeDtypeStruct(a.shape, a.dtype) for a in made],
            in_specs=[any_spec] * 4,
            out_specs=[any_spec] * 4,
            scratch_shapes=[pltpu.VMEM(a.shape, a.dtype) for a in made] + [dma((2, 4))],
        )(*made)
        weights = tuple(w.reshape(1, F * rows, cols) for w in (gate_out, up_out, down_out))
        return (*weights, mixed.T)

    in_specs = (
        P(("grp", "fs"), None),
        P(("grp", "fs"), None),
        P(("grp", "fs"), None),
        P("fs"),
        P(None, "fs", "tp"),
        P(None, "fs", "tp"),
        P(None, "fs", "tp"),
    )
    out_specs = (
        P(("grp", "fs"), None, "tp"),
        P(("grp", "fs"), None, "tp"),
        P(("grp", "fs"), None, "tp"),
        P(("grp", "fs"), "tp"),
    )
    return jax.shard_map(
        on_device, mesh=mesh, in_specs=in_specs, out_specs=out_specs, check_vma=False
    )
```
